128 devices in a mesh: ep: 16 (over z, x), tp: 8 (over y, core).
Axes of the slice: x: 4, y: 4, z: 4, core: 2. Of those that a mesh axis runs over, the one named last changes fastest.
Arguments:
- glu_value: bfloat16 [131072, 1024], P(('ep', 'tp')), may hold values from -6 to 6
- glu_gate: bfloat16 [131072, 1024], P(('ep', 'tp')), may hold values from -6 to 6
- conv_taps: float32 [31, 1024], replicated, may hold values from -12 to 12
- chan_gain: float32 [1024], replicated, may hold values from 0.1 to 1.9
- chan_shift: float32 [1024], replicated, may hold values from -3 to 3
- mix_out_weight: bfloat16 [1024, 2048], P('tp'), may hold values from -0.1875 to 0.1875
- moe_input: bfloat16 [16384, 2048], P(('ep', 'tp')), may hold values from -6 to 6
- moe_gain: float32 [2048], replicated, may hold values from 0.1 to 1.9
- expert_ids: int32 [16384, 4], P(('ep', 'tp')), may hold values from 0 to 127, all different within a row; in each aligned block of 128 rows (0 to 127, 128 to 255, ...) at most 5 rows name the same one
- expert_share: float32 [16384, 4], P(('ep', 'tp')), may hold values from 0.05 to 1
- expert_gate_weight: bfloat16 [128, 2048, 1024], P(('ep', 'tp')), may hold values from -0.375 to 0.375
- expert_up_weight: bfloat16 [128, 2048, 1024], P(('ep', 'tp')), may hold values from -0.375 to 0.375
- expert_down_weight: bfloat16 [128, 1024, 2048], P(('ep', 'tp')), may hold values from -0.0390625 to 0.0390625
Outputs:
- mixed: bfloat16 [131072, 2048], P(('ep', 'tp'))
- moe_output: bfloat16 [16384, 2048], P(('ep', 'tp'))
The draws below stay inside these ranges and needn't reach their ends.
Inputs may be any that keep to these rules, and one draw needn't show every extreme that they name: `expert_ids`: each row names 4 different experts. In each aligned block of 128 rows (the rows of one device) no expert is named by more than 5 rows, and in some block one expert is named by exactly 5 rows.
All inputs are finite; a program needn't handle non-finite values.
Results may differ from the reference program's by a relative error of at most 0.0071.
Values may be sent and summed in bfloat16 or wider, within the bound.
A program may use at most 192 MiB of HBM per device.

```python
import math
import jax
import jax.numpy as jnp
import numpy as np
from jax import lax

D = 2048
CW = 1024
KERNEL = 31
FF = 1024
TOP = 4
MOE_TOK = 128
EXPERTS = 128
CAP = 5
MIX_LEN = 131072
MOE_LEN = 16384
N_EP = 16
N_TP = 8


def draw_conv_taps(key, part):
    base_key = jax.random.fold_in(key, 11)
    tap_key, chan_key = jax.random.split(base_key)
    chan_scale = jnp.exp(jax.random.uniform(chan_key, (1, CW), jnp.float32, 0.0, 2.3))
    tap_values = jax.random.truncated_normal(tap_key, -4.0, 4.0, (KERNEL, CW), jnp.float32)
    return (tap_values * chan_scale * KERNEL ** (-0.5)).astype(jnp.float32)


def block_scale(rng, dims, shards, low, top_value):
    def one(position, blocks):
        draws = jax.random.uniform(jax.random.fold_in(jax.random.fold_in(rng, 6), position), (blocks,), jnp.float32, low / len(shards), top_value / len(shards))
        return jnp.repeat(jnp.exp(draws), dims[position] // blocks).reshape((-1,) + (1,) * (len(dims) - position - 1))

    factor_of = one(*shards[0])
    for cut in shards[1:]:
        factor_of = factor_of * one(*cut)
    return factor_of


def shared_out(own_key, own, number, rows, count, top, reach, slope):
    order = jax.random.permutation(own_key, count)
    crowded, ordinary = portions_of(count, rows * top, reach, slope, True), portions_of(count, rows * top, reach, slope, False)
    places = jnp.arange(count)

    def named(lengths, offset_by):
        used = int((lengths > 0).sum())
        fixed = max(1, used // 4)
        shifted = fixed + (places - fixed + offset_by * (used - fixed)) % max(1, count - fixed)
        return jnp.zeros((count,), jnp.int32).at[order[jnp.where(places < fixed, places, shifted)]].set(jnp.asarray(lengths, jnp.int32))

    lengths = jnp.where(number % 4 == 0, named(crowded, number // 4), named(ordinary, number - number // 4 - 1))
    mixed = jax.random.permutation(jax.random.fold_in(own, 3), count)
    source_of, sink = mixed[0:count // 2 * 2:2], mixed[1:count // 2 * 2:2]
    slack = jnp.minimum(lengths[source_of] - 1, reach - lengths[sink]) // 2
    slack = jnp.where((source_of == order[0]) | (sink == order[0]) | (lengths[sink] == 0), 0, jnp.maximum(slack, 0))
    shifted = jax.random.randint(jax.random.fold_in(own, 4), (count // 2,), 0, 1 << 20) % (slack + 1)
    lengths = lengths.at[source_of].add(-shifted).at[sink].add(shifted)
    labels = jnp.searchsorted(jnp.cumsum(lengths), jnp.arange(rows * top), side="right").astype(jnp.int32)
    listing = labels.reshape(top, rows).T
    listing = listing[jax.random.permutation(jax.random.fold_in(own, 1), rows)]
    offset_by = jax.random.randint(jax.random.fold_in(own, 2), (rows, 1), 0, top)
    return jnp.take_along_axis(listing, (jnp.arange(top)[None, :] + offset_by) % top, axis=1)


def portions_of(amount, total, reach, skew, full):
    portions = [(1 << 20) // math.isqrt(rank ** skew) + 1 for rank in range(1, amount + 1)]
    largest = reach if full else min(reach, max(-(-total // amount), total * portions[0] // sum(portions)))
    least = 1 if total - largest >= amount - 1 else 0
    given, surplus = [largest] + [least] * (amount - 1), total - largest - least * (amount - 1)
    while surplus > 0:
        movable = [i for i in range(1, amount) if given[i] < largest] or [i for i in range(1, amount) if given[i] < reach]
        pool, budget = sum([portions[i] for i in movable]), surplus
        for i in movable:
            more = min(reach - given[i], max(1, budget * portions[i] // pool), surplus)
            given[i] = given[i] + more
            surplus = surplus - more
    return np.array(given)


def centred(stream_key, dims, deviation, reach, shards=(), kind=jnp.bfloat16):
    loudness = block_scale(stream_key, dims, shards, -0.22, 0.18) if shards else 1.0
    array = jax.random.normal(stream_key, dims, jnp.float32) * deviation * loudness
    return jnp.minimum(jnp.maximum(array, -reach), reach).astype(kind)


def setup_inputs(seed: int = 0) -> dict:
    seeds = jax.random.split(jax.random.key(seed), 14)
    glu_value = centred(seeds[0], (MIX_LEN, CW), 1.0, 6.0, ((0, 128),))
    glu_gate = centred(seeds[1], (MIX_LEN, CW), 1.0, 6.0, ((0, 128),))
    conv_taps = draw_conv_taps(jax.random.fold_in(seeds[13], 71), 0)
    chan_gain = jnp.clip(1.0 + 0.18 * jax.random.normal(seeds[3], (CW,), jnp.float32), 0.1, 1.9)
    chan_shift = centred(seeds[4], (CW,), 0.5, 3.0, (), jnp.float32)
    mix_out_weight = centred(seeds[5], (CW, D), CW ** -0.5, 0.1875, ((0, 8),))
    moe_input = centred(seeds[6], (MOE_LEN, D), 1.0, 6.0, ((0, 128),))
    moe_gain = jnp.clip(1.0 + 0.18 * jax.random.normal(seeds[7], (D,), jnp.float32), 0.1, 1.9)
    expert_ids_keys = jax.random.split(jax.random.fold_in(seeds[8], 1), MOE_LEN // MOE_TOK)
    expert_ids_turns = jax.random.permutation(jax.random.fold_in(seeds[8], 3), MOE_LEN // MOE_TOK)
    expert_ids = jax.vmap(lambda own, number: shared_out(jax.random.fold_in(seeds[8], 2), own, number, MOE_TOK, EXPERTS, TOP, CAP, 1))(expert_ids_keys, expert_ids_turns).reshape((MOE_LEN, TOP))
    expert_share = jnp.clip(jnp.exp(math.log(1.0) - 2.9957323 * jax.random.uniform(seeds[9], (MOE_LEN, TOP), jnp.float32) ** block_scale(seeds[9], (MOE_LEN, TOP), ((0, 128),), -0.2, 0.2)), 0.05, 1.0)
    expert_gate_weight = centred(seeds[10], (EXPERTS, D, FF), (D // 9) ** -0.5, 0.375, ((0, 128),))
    expert_up_weight = centred(seeds[11], (EXPERTS, D, FF), (D // 9) ** -0.5, 0.375, ((0, 128),))
    expert_down_weight = centred(seeds[12], (EXPERTS, FF, D), (25 * FF) ** -0.5, 0.0390625, ((0, 128),))
    return {"glu_value": glu_value, "glu_gate": glu_gate, "conv_taps": conv_taps, "chan_gain": chan_gain, "chan_shift": chan_shift, "mix_out_weight": mix_out_weight, "moe_input": moe_input, "moe_gain": moe_gain, "expert_ids": expert_ids, "expert_share": expert_share, "expert_gate_weight": expert_gate_weight, "expert_up_weight": expert_up_weight, "expert_down_weight": expert_down_weight}


CLAMP_LIMIT = 7.0
GLU_SLOPE = 1.702

def expert_apply(flat_rows, gate_matrix, up_matrix, down_matrix):
    pre_gate = jnp.dot(flat_rows, gate_matrix, preferred_element_type=jnp.float32)
    pre_up = jnp.dot(flat_rows, up_matrix, preferred_element_type=jnp.float32)
    gated = jnp.minimum(pre_gate, CLAMP_LIMIT)
    lifted = jnp.clip(pre_up, -CLAMP_LIMIT, CLAMP_LIMIT) + 1.0
    hidden = (lifted * gated * jax.nn.sigmoid(GLU_SLOPE * gated)).astype(jnp.bfloat16)
    return jnp.dot(hidden, down_matrix, preferred_element_type=jnp.float32).astype(jnp.bfloat16)

def reference(glu_value, glu_gate, conv_taps, chan_gain, chan_shift, mix_out_weight, moe_input, moe_gain, expert_ids, expert_share, expert_gate_weight, expert_up_weight, expert_down_weight):
    gated_input = glu_value.astype(jnp.float32) * jax.nn.sigmoid(glu_gate.astype(jnp.float32))
    padded = jnp.concatenate([jnp.zeros((KERNEL - 1, CW), jnp.float32), gated_input], 0)
    convolved = jnp.zeros((MIX_LEN, CW), jnp.float32)
    for offset in range(KERNEL):
        convolved = convolved + conv_taps[offset] * padded[offset:offset + MIX_LEN]
    center = lax.optimization_barrier(jnp.mean(convolved, axis=-1, keepdims=True))
    spread = lax.optimization_barrier(jnp.mean(jnp.square(convolved - center), axis=-1, keepdims=True))
    normalized = (convolved - center) * lax.rsqrt(spread + 1e-05) * chan_gain + chan_shift
    activated = jax.nn.silu(normalized).astype(jnp.bfloat16)
    mixed = jnp.dot(activated, mix_out_weight, preferred_element_type=jnp.float32).astype(jnp.bfloat16)
    features = moe_input.astype(jnp.float32)
    scaled = features * lax.rsqrt(lax.optimization_barrier(jnp.mean(jnp.square(features), axis=-1, keepdims=True)) + 1e-06)
    moe_normed = (scaled * moe_gain).astype(jnp.bfloat16)
    flat_ids = expert_ids.reshape(-1)
    flat_share = expert_share.reshape(-1)
    slots = N_EP * N_TP * CAP

    def one_expert(total, inputs):
        number, gate_matrix, up_matrix, down_matrix = inputs
        chosen = flat_ids == number
        picked = jnp.nonzero(chosen, size=slots, fill_value=0)[0].astype(jnp.int32)
        live = jnp.arange(slots, dtype=jnp.int32) < jnp.sum(chosen.astype(jnp.int32))
        token_rows = (picked // TOP).astype(jnp.int32)
        answers = expert_apply(moe_normed[token_rows], gate_matrix, up_matrix, down_matrix)
        weights = jnp.where(live, flat_share[picked], jnp.zeros((), flat_share.dtype))
        total = total.at[token_rows].add(weights[:, None] * answers.astype(jnp.float32))
        return (total, number)
    numbers = jnp.arange(EXPERTS, dtype=jnp.int32)
    total, unused = lax.scan(one_expert, jnp.zeros((MOE_LEN, D), jnp.float32), (numbers, expert_gate_weight, expert_up_weight, expert_down_weight))
    return (mixed, total.astype(jnp.bfloat16))
```

```python
import functools

import jax
import jax.numpy as jnp
from jax import lax
from jax.experimental import pallas as pl
from jax.experimental.pallas import tpu as pltpu
from jax.sharding import PartitionSpec as P

MESH = pl.DeviceIdType.MESH
F32 = jnp.float32
BF16 = jnp.bfloat16
CLAMP_LIMIT = 7.0
GLU_SLOPE = 1.702
CAP = 5
PEERS = 128
SCRAMBLE = 101
GROUPS = 4
GSIZE = PEERS // GROUPS
PIECES = 16
BLOCK = CAP * PIECES
PITCH = 88
HALO = 32
SEGMENT = 129
CONV_STEP = 12
CONV_BLOCKS = -(-SEGMENT // CONV_STEP)


def sigmoid(v):
    return 0.5 + 0.5 * jnp.tanh(0.5 * v)


def displacement(i):
    j = (i * SCRAMBLE) % PEERS
    return j // 32, (j // 8) % 4, (j // 2) % 4, j % 2


def kernel(
    value_hbm, gate_hbm, taps_ref, cgain_ref, cshift_ref, wout_hbm, moe_hbm, mgain_ref, ids_ref, share_ref,
    wg_hbm, wu_hbm, wd_hbm,
    mixed_hbm, moe_out_hbm,
    value, gate, halo, glu, conv, act, wfull, obuf,
    xin, xn, rankm, sharem, sbuf, abuf, rbuf, tbuf, scr, rows, hidden, wg, wu, wd, result, mout,
    local_sem, out_sem, halo_send, halo_recv, w_send, w_recv, wf_send, wf_recv,
    d_send, d_recv, r_send, r_recv, self_sem,
):
    ep = lax.axis_index("ep")
    tp = lax.axis_index("tp")
    me = ep * 8 + tp
    z, x, y, c = ep // 4, ep % 4, tp // 2, tp % 2

    def device(dz, dx, dy, dc):
        return ((z + dz + 4) % 4) * 4 + (x + dx + 4) % 4, ((y + dy + 4) % 4) * 2 + (c + dc) % 2

    barrier = pltpu.get_barrier_semaphore()

    def hello(i, carry):
        target = device(*displacement(i))
        pl.semaphore_signal(barrier, inc=1, device_id=target, device_id_type=MESH)
        return carry

    lax.fori_loop(1, PEERS, hello, 0)

    load_moe = pltpu.make_async_copy(moe_hbm, xin, local_sem.at[0])
    load_w = pltpu.make_async_copy(wout_hbm, wfull.at[pl.ds(pl.multiple_of(tp * 128, 128), 128), :], local_sem.at[1])
    load_value = pltpu.make_async_copy(value_hbm, value, local_sem.at[2])
    load_gate = pltpu.make_async_copy(gate_hbm, gate, local_sem.at[3])
    load_wg = pltpu.make_async_copy(wg_hbm.at[0], wg, local_sem.at[4])
    load_wu = pltpu.make_async_copy(wu_hbm.at[0], wu, local_sem.at[5])
    load_wd = pltpu.make_async_copy(wd_hbm.at[0], wd, local_sem.at[6])
    for load in (load_moe, load_value, load_gate, load_w, load_wg, load_wu, load_wd):
        load.start()

    lane = lax.broadcasted_iota(jnp.int32, (128, PEERS), 1)
    row = lax.broadcasted_iota(jnp.int32, (128, PEERS), 0)
    j = (lane * SCRAMBLE) & 127
    expert = (
        (((z + (j >> 5)) & 3) * 32) + (((x + (j >> 3)) & 3) * 8) + (((y + (j >> 1)) & 3) * 2) + ((c + j) & 1)
    )
    chosen = jnp.zeros((128, PEERS), F32)
    shares = jnp.zeros((128, PEERS), F32)
    for k in range(4):
        hit = ids_ref[:, k : k + 1] == expert
        chosen = jnp.where(hit, 1.0, chosen)
        shares = jnp.where(hit, share_ref[:, k : k + 1], shares)
    before = jnp.where(row > lane, 1.0, 0.0).astype(BF16)
    rank = jnp.dot(before, chosen.astype(BF16), preferred_element_type=F32)
    rankm[...] = jnp.where(chosen > 0.5, rank, -1.0)
    sharem[...] = shares

    load_moe.wait()

    def norm_rows(b, carry):
        at = pl.ds(pl.multiple_of(b * 32, 32), 32)
        f = xin[at, :].astype(F32)
        scaled = f * lax.rsqrt(jnp.mean(f * f, axis=-1, keepdims=True) + 1e-06)
        xn[at, :] = (scaled * mgain_ref[...]).astype(BF16)
        return carry

    lax.fori_loop(0, 4, norm_rows, 0)

    def pack(dst, first):
        def one(i, carry):
            dst[first + i] = scr[pl.ds(pl.multiple_of(i * PITCH, 8), BLOCK), :].astype(BF16)
            return carry

        lax.fori_loop(0, GSIZE, one, 0, unroll=4)

    def unpack(src, first):
        def one(i, carry):
            scr[pl.ds(pl.multiple_of(i * PITCH, 8), BLOCK), :] = src[first + i].astype(F32)
            return carry

        lax.fori_loop(0, GSIZE, one, 0, unroll=4)

    def gather(g):
        for r in range(CAP):
            take = jnp.where(rankm[...] == float(r), 1.0, 0.0).astype(BF16)[:, g * GSIZE : (g + 1) * GSIZE]

            def some(n, carry, take=take, r=r):
                cols = pl.ds(pl.multiple_of(n * 512, 512), 512)
                got = lax.dot_general(take, xn[:, cols], (((0,), (0,)), ((), ())), preferred_element_type=F32)
                for q in range(4):
                    scr[pl.ds(r * PIECES + n * 4 + q, GSIZE, stride=PITCH), :] = got[:, q * 128 : (q + 1) * 128]
                return carry

            lax.fori_loop(0, 4, some, 0)
        pack(sbuf, g * GSIZE)

    def send_group(g):
        def one(i, carry):
            pltpu.make_async_remote_copy(
                src_ref=sbuf.at[i], dst_ref=abuf.at[i], send_sem=d_send, recv_sem=d_recv.at[g],
                device_id=device(*displacement(i)), device_id_type=MESH,
            ).start()
            return carry

        lax.fori_loop(max(1, g * GSIZE), (g + 1) * GSIZE, one, 0)

    gather(0)
    load_value.wait()
    load_gate.wait()
    load_w.wait()
    pl.semaphore_wait(barrier, PEERS - 1)

    nxt = (me + 1) % 128
    halo_copies = []
    for n, half in enumerate((value, gate)):
        cp = pltpu.make_async_remote_copy(
            src_ref=half.at[pl.ds(1024 - HALO, HALO), :], dst_ref=halo.at[n],
            send_sem=halo_send.at[n], recv_sem=halo_recv.at[n],
            device_id=(nxt // 8, nxt % 8), device_id_type=MESH,
        )
        cp.start()
        halo_copies.append(cp)
    self_copy = pltpu.make_async_copy(sbuf.at[0], abuf.at[0], self_sem.at[0])
    self_copy.start()
    send_group(0)
    for g in range(1, GROUPS):
        gather(g)
        send_group(g)

    mine = wfull.at[pl.ds(pl.multiple_of(tp * 128, 128), 128), :]
    w_copies = []
    for d in range(1, 4):
        cp = pltpu.make_async_remote_copy(
            src_ref=mine, dst_ref=mine, send_sem=w_send.at[d - 1], recv_sem=w_recv.at[d - 1],
            device_id=device(0, 0, d, 0), device_id_type=MESH,
        )
        cp.start()
        w_copies.append(cp)
    wf_copies = []

    def forward(d):
        origin = ((y - d + 4) % 4) * 2 + c
        block = wfull.at[pl.ds(pl.multiple_of(origin * 128, 128), 128), :]
        cp = pltpu.make_async_remote_copy(
            src_ref=block, dst_ref=block, send_sem=wf_send.at[d], recv_sem=wf_recv.at[d],
            device_id=device(0, 0, 0, 1), device_id_type=MESH,
        )
        cp.start()
        wf_copies.append(cp)

    forward(0)

    def glu_rows(b, carry):
        at = pl.ds(pl.multiple_of(b * 32, 32), 32)
        to = pl.ds(pl.multiple_of(b * 32 + HALO, 32), 32)
        gated = value[at, :].astype(F32) * sigmoid(gate[at, :].astype(F32))
        for l in range(8):
            glu[l, to, :] = gated[:, l * 128 : (l + 1) * 128]
        return carry

    lax.fori_loop(0, 1024 // 32, glu_rows, 0)
    for cp in halo_copies:
        cp.wait()
    border = halo[0].astype(F32) * sigmoid(halo[1].astype(F32))
    border = border * jnp.minimum(me, 1).astype(F32)
    for l in range(8):
        glu[l, pl.ds(0, HALO), :] = border[:, l * 128 : (l + 1) * 128]
        glu[l, pl.ds(1024 + HALO, 8), :] = jnp.zeros((8, 128), F32)

    def conv_block(n, carry):
        l, block = n // CONV_BLOCKS, n % CONV_BLOCKS
        lanes = pl.ds(pl.multiple_of(l * 128, 128), 128)
        b0 = jnp.minimum(block * CONV_STEP, SEGMENT - CONV_STEP)
        near = [glu[l, pl.ds(b0 + 2 + u, 8, stride=SEGMENT), :] for u in range(CONV_STEP + 30)]
        totals = [None] * CONV_STEP
        for tap in range(31):
            w = jnp.broadcast_to(taps_ref[tap : tap + 1, lanes], (8, 128))
            for b in range(CONV_STEP):
                term = w * near[b + tap]
                totals[b] = term if tap == 0 else totals[b] + term
        for b in range(CONV_STEP):
            conv[l, pl.ds(b0 + b, 8, stride=SEGMENT), :] = totals[b]
        return carry

    lax.fori_loop(0, 8 * CONV_BLOCKS, conv_block, 0)

    def norm_conv(n, carry):
        at = pl.ds(pl.multiple_of(n * 32, 32), 32)
        v = jnp.concatenate([conv[l, at, :] for l in range(8)], axis=-1)
        center = jnp.mean(v, axis=-1, keepdims=True)
        v = v - center
        spread = jnp.mean(v * v, axis=-1, keepdims=True)
        u = v * lax.rsqrt(spread + 1e-05) * cgain_ref[...] + cshift_ref[...]
        act[at, :] = (u * sigmoid(u)).astype(BF16)
        return carry

    lax.fori_loop(0, 32, norm_conv, 0, unroll=2)

    load_wg.wait()
    load_wu.wait()
    load_wd.wait()

    def group_wait(buf, sem, g):
        n = GSIZE - 1 if g == 0 else GSIZE
        pltpu.make_async_copy(buf.at[pl.ds(0, n)], buf.at[pl.ds(0, n)], sem.at[g]).wait()

    def experts(g):
        unpack(abuf, g * GSIZE)

        def line_up(n, carry):
            cols = pl.ds(pl.multiple_of(n * 128, 128), 128)
            for r in range(CAP):
                rows[pl.ds(r * GSIZE, GSIZE), cols] = scr[pl.ds(r * PIECES + n, GSIZE, stride=PITCH), :].astype(BF16)
            return carry

        lax.fori_loop(0, PIECES, line_up, 0)

        def up(n, carry):
            cols = pl.ds(pl.multiple_of(n * 256, 256), 256)
            pre_gate = jnp.dot(rows[...], wg[:, cols], preferred_element_type=F32)
            pre_up = jnp.dot(rows[...], wu[:, cols], preferred_element_type=F32)
            gated = jnp.minimum(pre_gate, CLAMP_LIMIT)
            lifted = jnp.clip(pre_up, -CLAMP_LIMIT, CLAMP_LIMIT) + 1.0
            hidden[:, cols] = (lifted * gated * sigmoid(GLU_SLOPE * gated)).astype(BF16)
            return carry

        lax.fori_loop(0, 4, up, 0)

        def down(n, carry):
            cols = pl.ds(pl.multiple_of(n * 256, 256), 256)
            got = jnp.dot(hidden[...], wd[:, cols], preferred_element_type=F32)
            for r in range(CAP):
                for q in range(2):
                    scr[pl.ds(r * PIECES + n * 2 + q, GSIZE, stride=PITCH), :] = got[
                        r * GSIZE : (r + 1) * GSIZE, q * 128 : (q + 1) * 128
                    ]
            return carry

        lax.fori_loop(0, 8, down, 0)
        pack(rbuf, g * GSIZE)

        def give_back(i, carry):
            dz, dx, dy, dc = displacement(i)
            pltpu.make_async_remote_copy(
                src_ref=rbuf.at[i], dst_ref=tbuf.at[i], send_sem=r_send, recv_sem=r_recv.at[g],
                device_id=device(-dz, -dx, -dy, dc), device_id_type=MESH,
            ).start()
            return carry

        lax.fori_loop(max(1, g * GSIZE), (g + 1) * GSIZE, give_back, 0)

    self_copy.wait()
    for g in range(GROUPS):
        group_wait(abuf, d_recv, g)
        experts(g)
    self_back = pltpu.make_async_copy(rbuf.at[0], tbuf.at[0], self_sem.at[1])
    self_back.start()

    for d in range(1, 4):
        w_copies[d - 1].wait()
        forward(d)
    for cp in wf_copies:
        cp.wait()

    def project(m, carry):
        at = pl.ds(pl.multiple_of(m * 256, 256), 256)

        def part(n, inner):
            cols = pl.ds(pl.multiple_of(n * 512, 512), 512)
            obuf[at, cols] = jnp.dot(act[at, :], wfull[:, cols], preferred_element_type=F32).astype(BF16)
            return inner

        lax.fori_loop(0, 4, part, 0)
        return carry

    lax.fori_loop(0, 4, project, 0)
    store_mixed = pltpu.make_async_copy(obuf, mixed_hbm, out_sem.at[0])
    store_mixed.start()

    self_back.wait()
    for g in range(GROUPS):
        group_wait(tbuf, r_recv, g)
        unpack(tbuf, g * GSIZE)

        def line_up_back(n, carry, g=g):
            cols = pl.ds(pl.multiple_of(n * 128, 128), 128)
            for r in range(CAP):
                result[pl.ds(r * PEERS + g * GSIZE, GSIZE), cols] = scr[
                    pl.ds(r * PIECES + n, GSIZE, stride=PITCH), :
                ].astype(BF16)
            return carry

        lax.fori_loop(0, PIECES, line_up_back, 0)
    weights = jnp.concatenate(
        [jnp.where(rankm[...] == float(r), sharem[...], 0.0).astype(BF16) for r in range(CAP)], axis=1
    )

    def combine(n, carry):
        cols = pl.ds(pl.multiple_of(n * 512, 512), 512)
        mout[:, cols] = jnp.dot(weights, result[:, cols], preferred_element_type=F32).astype(BF16)
        return carry

    lax.fori_loop(0, 4, combine, 0)
    store_moe = pltpu.make_async_copy(mout, moe_out_hbm, out_sem.at[1])
    store_moe.start()
    sent = sbuf.at[pl.ds(0, PEERS - 1)]
    pltpu.make_async_copy(sent, sent, d_send).wait()
    pltpu.make_async_copy(sent, sent, r_send).wait()
    store_mixed.wait()
    store_moe.wait()


def body(
    glu_value, glu_gate, conv_taps, chan_gain, chan_shift, mix_out_weight, moe_input, moe_gain, expert_ids,
    expert_share, expert_gate_weight, expert_up_weight, expert_down_weight,
):
    hbm = pl.BlockSpec(memory_space=pl.ANY)
    vmem = pl.BlockSpec(memory_space=pltpu.VMEM)
    dma = pltpu.SemaphoreType.DMA
    return pl.pallas_call(
        kernel,
        out_shape=(
            jax.ShapeDtypeStruct((1024, 2048), BF16),
            jax.ShapeDtypeStruct((128, 2048), BF16),
        ),
        in_specs=[hbm, hbm, vmem, vmem, vmem, hbm, hbm, vmem, vmem, vmem, hbm, hbm, hbm],
        out_specs=(hbm, hbm),
        scratch_shapes=[
            pltpu.VMEM((1024, 1024), BF16),
            pltpu.VMEM((1024, 1024), BF16),
            pltpu.VMEM((2, HALO, 1024), BF16),
            pltpu.VMEM((8, 1024 + HALO + 8, 128), F32),
            pltpu.VMEM((8, 8 * SEGMENT, 128), F32),
            pltpu.VMEM((1024, 1024), BF16),
            pltpu.VMEM((1024, 2048), BF16),
            pltpu.VMEM((1024, 2048), BF16),
            pltpu.VMEM((128, 2048), BF16),
            pltpu.VMEM((128, 2048), BF16),
            pltpu.VMEM((128, PEERS), F32),
            pltpu.VMEM((128, PEERS), F32),
            pltpu.VMEM((PEERS, BLOCK, 128), BF16),
            pltpu.VMEM((PEERS, BLOCK, 128), BF16),
            pltpu.VMEM((PEERS, BLOCK, 128), BF16),
            pltpu.VMEM((PEERS, BLOCK, 128), BF16),
            pltpu.VMEM((GSIZE * PITCH, 128), F32),
            pltpu.VMEM((GSIZE * CAP, 2048), BF16),
            pltpu.VMEM((GSIZE * CAP, 1024), BF16),
            pltpu.VMEM((2048, 1024), BF16),
            pltpu.VMEM((2048, 1024), BF16),
            pltpu.VMEM((1024, 2048), BF16),
            pltpu.VMEM((PEERS * CAP, 2048), BF16),
            pltpu.VMEM((128, 2048), BF16),
            dma((7,)), dma((2,)), dma((2,)), dma((2,)), dma((3,)), dma((3,)), dma((4,)), dma((4,)),
            dma, dma((GROUPS,)), dma, dma((GROUPS,)), dma((2,)),
        ],
        compiler_params=pltpu.CompilerParams(
            collective_id=0, has_side_effects=True, vmem_limit_bytes=62 * 2**20
        ),
        name="mixer",
    )(
        glu_value, glu_gate, conv_taps, chan_gain.reshape(1, -1), chan_shift.reshape(1, -1), mix_out_weight,
        moe_input, moe_gain.reshape(1, -1), expert_ids, expert_share,
        expert_gate_weight, expert_up_weight, expert_down_weight,
    )


def solution(mesh):
    both = ("ep", "tp")
    placed = (
        P(both, None), P(both, None), P(), P(), P(), P("tp", None), P(both, None), P(), P(both, None),
        P(both, None), P(both, None, None), P(both, None, None), P(both, None, None),
    )
    return jax.shard_map(
        body,
        mesh=mesh,
        in_specs=placed,
        out_specs=(P(both, None), P(both, None)),
        check_vma=False,
    )
```

```python
import functools

import jax
import jax.numpy as jnp
from jax import lax
from jax.experimental import pallas as pl
from jax.experimental.pallas import tpu as pltpu
from jax.sharding import PartitionSpec as P

MESH = pl.DeviceIdType.MESH
F32 = jnp.float32
BF16 = jnp.bfloat16
CLAMP_LIMIT = 7.0
GLU_SLOPE = 1.702
CAP = 5
PEERS = 128
SCRAMBLE = 101
GROUPS = 4
GSIZE = PEERS // GROUPS
PIECES = 16
BLOCK = CAP * PIECES
PITCH = 88
HALO = 32
SEGMENT = 129
CONV_STEP = 12
CONV_BLOCKS = -(-SEGMENT // CONV_STEP)


def sigmoid(v):
    return 0.5 + 0.5 * jnp.tanh(0.5 * v)


def displacement(i):
    j = (i * SCRAMBLE) & (PEERS - 1)
    return j >> 5, j >> 3, j >> 1, j


def kernel(
    value_hbm, gate_hbm, taps_hbm, cgain_hbm, cshift_hbm, wout_hbm, moe_hbm, mgain_hbm, ids_hbm, share_hbm,
    wg_hbm, wu_hbm, wd_hbm,
    mixed_hbm, moe_out_hbm,
    taps_ref, cgain_ref, cshift_ref, mgain_ref, ids_ref, share_ref, value, gate, halo, glu, conv, act, wfull, obuf,
    xin, xn, rankm, sharem, sbuf, abuf, rbuf, tbuf, scr, rows, hidden, wg, wu, wd, result, weights, mout,
    local_sem, out_sem, halo_send, halo_recv, w_send, w_recv, own_send, own_recv,
    d_send, d_recv, r_send, r_recv, self_sem,
):
    ep = lax.axis_index("ep")
    tp = lax.axis_index("tp")
    me = ep * 8 + tp
    z, x, y, c = ep >> 2, ep & 3, tp >> 1, tp & 1

    def device(dz, dx, dy, dc):
        return ((z + dz) & 3) * 4 + ((x + dx) & 3), ((y + dy) & 3) * 2 + ((c + dc) & 1)

    barrier = pltpu.get_barrier_semaphore()

    def hello(i, carry):
        pl.semaphore_signal(barrier, inc=1, device_id=device(*displacement(i)), device_id_type=MESH)
        return carry

    lax.fori_loop(1, PEERS, hello, 0, unroll=3)

    shard = pl.ds(pl.multiple_of(tp * 128, 128), 128)
    pairs = (
        (ids_hbm, ids_ref), (share_hbm, share_ref), (mgain_hbm, mgain_ref),
        (taps_hbm, taps_ref), (cgain_hbm, cgain_ref), (cshift_hbm, cshift_ref),
    )
    small = [pltpu.make_async_copy(a, b, local_sem.at[15 + n]) for n, (a, b) in enumerate(pairs)]
    load_moe = pltpu.make_async_copy(moe_hbm, xin, local_sem.at[0])
    load_w = [
        pltpu.make_async_copy(wout_hbm.at[:, pl.ds(n * 256, 256)], wfull.at[n, shard, :], local_sem.at[7 + n])
        for n in range(8)
    ]
    load_value = pltpu.make_async_copy(value_hbm, value, local_sem.at[2])
    load_gate = pltpu.make_async_copy(gate_hbm, gate, local_sem.at[3])
    load_wg = pltpu.make_async_copy(wg_hbm.at[0], wg, local_sem.at[4])
    load_wu = pltpu.make_async_copy(wu_hbm.at[0], wu, local_sem.at[5])
    load_wd = pltpu.make_async_copy(wd_hbm.at[0], wd, local_sem.at[6])
    for load in (*small, load_moe, *load_w, load_value, load_gate, load_wg, load_wu, load_wd):
        load.start()

    for load in small:
        load.wait()

    lane = lax.broadcasted_iota(jnp.int32, (PEERS, 128), 1)
    row = lax.broadcasted_iota(jnp.int32, (PEERS, 128), 0)
    j = (row * SCRAMBLE) & 127
    expert = (
        (((z + (j >> 5)) & 3) * 32) + (((x + (j >> 3)) & 3) * 8) + (((y + (j >> 1)) & 3) * 2) + ((c + j) & 1)
    )
    chosen = jnp.zeros((PEERS, 128), F32)
    shares = jnp.zeros((PEERS, 128), F32)
    for k in range(4):
        hit = ids_ref[k : k + 1, :] == expert
        chosen = jnp.where(hit, 1.0, chosen)
        shares = jnp.where(hit, share_ref[k : k + 1, :], shares)
    before = jnp.where(row < lane, 1.0, 0.0).astype(BF16)
    rank = jnp.dot(chosen.astype(BF16), before, preferred_element_type=F32)
    rankm[...] = jnp.where(chosen > 0.5, rank, -1.0)
    sharem[...] = shares

    load_moe.wait()

    def norm_rows(b, carry):
        at = pl.ds(pl.multiple_of(b * 32, 32), 32)
        f = xin[at, :].astype(F32)
        scaled = f * lax.rsqrt(jnp.mean(f * f, axis=-1, keepdims=True) + 1e-06)
        xn[at, :] = (scaled * mgain_ref[...]).astype(BF16)
        return carry

    lax.fori_loop(0, 4, norm_rows, 0)

    def pack(dst, first):
        def one(i, carry):
            dst[first + i] = scr[pl.ds(pl.multiple_of(i * PITCH, 8), BLOCK), :].astype(BF16)
            return carry

        lax.fori_loop(0, GSIZE, one, 0, unroll=4)

    def unpack(src, first):
        def one(i, carry):
            scr[pl.ds(pl.multiple_of(i * PITCH, 8), BLOCK), :] = src[first + i].astype(F32)
            return carry

        lax.fori_loop(0, GSIZE, one, 0, unroll=4)

    def spread(got, first):
        for r in range(CAP):
            for q in range(4):
                scr[pl.ds(r * PIECES + first + q, GSIZE, stride=PITCH), :] = got[
                    r * GSIZE : (r + 1) * GSIZE, q * 128 : (q + 1) * 128
                ]

    def gather(g, carry):
        ranks = rankm[pl.ds(pl.multiple_of(g * GSIZE, GSIZE), GSIZE), :]
        take = jnp.concatenate([jnp.where(ranks == float(r), 1.0, 0.0) for r in range(CAP)], axis=0).astype(BF16)
        for n in range(4):
            spread(jnp.dot(take, xn[:, n * 512 : (n + 1) * 512], preferred_element_type=F32), n * 4)
        pack(sbuf, g * GSIZE)
        return carry

    lax.fori_loop(0, GROUPS, gather, 0)
    load_value.wait()
    load_gate.wait()
    for load in load_w:
        load.wait()
    pl.semaphore_wait(barrier, PEERS - 1)

    nxt = (me + 1) & 127
    halo_copies = []
    for n, half in enumerate((value, gate)):
        cp = pltpu.make_async_remote_copy(
            src_ref=half.at[pl.ds(1024 - HALO, HALO), :], dst_ref=halo.at[n],
            send_sem=halo_send.at[n], recv_sem=halo_recv.at[n],
            device_id=(nxt >> 3, nxt & 7), device_id_type=MESH,
        )
        cp.start()
        halo_copies.append(cp)

    def w_block(n, rows_at, stage, target):
        pltpu.make_async_remote_copy(
            src_ref=wfull.at[n, rows_at, :], dst_ref=wfull.at[n, rows_at, :],
            send_sem=w_send.at[stage], recv_sem=w_recv.at[stage], device_id=target, device_id_type=MESH,
        ).start()

    def w_wait(sem, blocks):
        some = obuf.at[pl.ds(0, 16 * blocks), :]
        pltpu.make_async_copy(some, some, sem).wait()

    def origin(d):
        return pl.ds(pl.multiple_of((((y - d) & 3) * 2 + c) * 128, 128), 128)

    for d in range(1, 4):
        w_block(x, shard, 0, device(0, 0, d, 0))
        w_block(4 + z, shard, 0, device(0, 0, d, 0))
    own_forward = pltpu.make_async_remote_copy(
        src_ref=wfull.at[:, shard, :], dst_ref=wfull.at[:, shard, :], send_sem=own_send, recv_sem=own_recv,
        device_id=device(0, 0, 0, 1), device_id_type=MESH,
    )
    own_forward.start()

    self_copy = pltpu.make_async_copy(sbuf.at[0], abuf.at[0], self_sem.at[0])
    self_copy.start()

    def send_group(g):
        def send(i, carry):
            pltpu.make_async_remote_copy(
                src_ref=sbuf.at[i], dst_ref=abuf.at[i], send_sem=d_send, recv_sem=d_recv.at[g],
                device_id=device(*displacement(i)), device_id_type=MESH,
            ).start()
            return carry

        lax.fori_loop(max(1, g * GSIZE), (g + 1) * GSIZE, send, 0)

    send_group(0)
    send_group(1)

    def glu_rows(b, carry):
        at = pl.ds(pl.multiple_of(b * 32, 32), 32)
        to = pl.ds(pl.multiple_of(b * 32 + HALO, 32), 32)
        gated = value[at, :].astype(F32) * sigmoid(gate[at, :].astype(F32))
        for l in range(8):
            glu[l, to, :] = gated[:, l * 128 : (l + 1) * 128]
        return carry

    lax.fori_loop(0, 1024 // 32, glu_rows, 0)
    for cp in halo_copies:
        cp.wait()
    border = halo[0].astype(F32) * sigmoid(halo[1].astype(F32))
    border = border * jnp.minimum(me, 1).astype(F32)
    for l in range(8):
        glu[l, pl.ds(0, HALO), :] = border[:, l * 128 : (l + 1) * 128]
        glu[l, pl.ds(1024 + HALO, 8), :] = jnp.zeros((8, 128), F32)

    def conv_block(n, carry):
        l, block = n // CONV_BLOCKS, n % CONV_BLOCKS
        lanes = pl.ds(pl.multiple_of(l * 128, 128), 128)
        b0 = jnp.minimum(block * CONV_STEP, SEGMENT - CONV_STEP)
        near = [glu[l, pl.ds(b0 + 2 + u, 8, stride=SEGMENT), :] for u in range(CONV_STEP + 30)]
        totals = [None] * CONV_STEP
        for tap in range(31):
            w = jnp.broadcast_to(taps_ref[tap : tap + 1, lanes], (8, 128))
            for b in range(CONV_STEP):
                term = w * near[b + tap]
                totals[b] = term if tap == 0 else totals[b] + term
        for b in range(CONV_STEP):
            conv[l, pl.ds(b0 + b, 8, stride=SEGMENT), :] = totals[b]
        return carry

    lax.fori_loop(0, 8 * CONV_BLOCKS, conv_block, 0)

    w_wait(w_recv.at[0], 6)
    for d in range(1, 4):
        for e in range(1, 4):
            w_block(x, origin(d), 1, device(0, e, 0, 0))
            w_block(4 + z, origin(d), 1, device(e, 0, 0, 0))
    send_group(2)
    send_group(3)

    def norm_conv(n, carry):
        at = pl.ds(pl.multiple_of(n * 32, 32), 32)
        v = jnp.concatenate([conv[l, at, :] for l in range(8)], axis=-1)
        center = jnp.mean(v, axis=-1, keepdims=True)
        v = v - center
        spread = jnp.mean(v * v, axis=-1, keepdims=True)
        u = v * lax.rsqrt(spread + 1e-05) * cgain_ref[...] + cshift_ref[...]
        act[at, :] = (u * sigmoid(u)).astype(BF16)
        return carry

    lax.fori_loop(0, 32, norm_conv, 0, unroll=2)

    load_wg.wait()
    load_wu.wait()
    load_wd.wait()

    def group_wait(buf, sem, g):
        n = GSIZE - 1 if g == 0 else GSIZE
        pltpu.make_async_copy(buf.at[pl.ds(0, n)], buf.at[pl.ds(0, n)], sem.at[g]).wait()

    def experts(g):
        unpack(abuf, g * GSIZE)

        def line_up(n, carry):
            cols = pl.ds(pl.multiple_of(n * 128, 128), 128)
            for r in range(CAP):
                rows[pl.ds(r * GSIZE, GSIZE), cols] = scr[pl.ds(r * PIECES + n, GSIZE, stride=PITCH), :].astype(BF16)
            return carry

        lax.fori_loop(0, PIECES, line_up, 0)

        def up(n, carry):
            cols = pl.ds(pl.multiple_of(n * 512, 512), 512)
            pre_gate = jnp.dot(rows[...], wg[:, cols], preferred_element_type=F32)
            pre_up = jnp.dot(rows[...], wu[:, cols], preferred_element_type=F32)
            gated = jnp.minimum(pre_gate, CLAMP_LIMIT)
            lifted = jnp.clip(pre_up, -CLAMP_LIMIT, CLAMP_LIMIT) + 1.0
            hidden[:, cols] = (lifted * gated * sigmoid(GLU_SLOPE * gated)).astype(BF16)
            return carry

        lax.fori_loop(0, 2, up, 0)

        def down(n, carry):
            cols = pl.ds(pl.multiple_of(n * 512, 512), 512)
            spread(jnp.dot(hidden[...], wd[:, cols], preferred_element_type=F32), n * 4)
            return carry

        lax.fori_loop(0, 4, down, 0)
        pack(rbuf, g * GSIZE)

        def give_back(i, carry):
            dz, dx, dy, dc = displacement(i)
            pltpu.make_async_remote_copy(
                src_ref=rbuf.at[i], dst_ref=tbuf.at[i], send_sem=r_send, recv_sem=r_recv.at[g],
                device_id=device(-dz, -dx, -dy, dc), device_id_type=MESH,
            ).start()
            return carry

        lax.fori_loop(max(1, g * GSIZE), (g + 1) * GSIZE, give_back, 0)

    self_copy.wait()
    for g in range(GROUPS):
        group_wait(abuf, d_recv, g)
        experts(g)
    self_back = pltpu.make_async_copy(rbuf.at[0], tbuf.at[0], self_sem.at[1])
    self_back.start()

    for r in range(CAP):
        weights[:, r * PEERS : (r + 1) * PEERS] = jnp.where(rankm[...] == float(r), sharem[...], 0.0).T.astype(BF16)

    w_wait(w_recv.at[1], 18)
    for d in range(1, 4):
        pltpu.make_async_remote_copy(
            src_ref=wfull.at[:, origin(d), :], dst_ref=wfull.at[:, origin(d), :],
            send_sem=w_send.at[2], recv_sem=w_recv.at[2], device_id=device(0, 0, 0, 1), device_id_type=MESH,
        ).start()
    own_forward.wait()
    w_wait(w_recv.at[2], 24)

    def project(n, carry):
        cols = pl.ds(pl.multiple_of(n * 256, 256), 256)
        for m in range(2):
            at = pl.ds(m * 512, 512)
            obuf[at, cols] = jnp.dot(act[at, :], wfull[n], preferred_element_type=F32).astype(BF16)
        return carry

    lax.fori_loop(0, 8, project, 0)
    store_mixed = pltpu.make_async_copy(obuf, mixed_hbm, out_sem.at[0])
    store_mixed.start()

    self_back.wait()
    for g in range(GROUPS):
        group_wait(tbuf, r_recv, g)
        unpack(tbuf, g * GSIZE)

        def line_up_back(n, carry, g=g):
            cols = pl.ds(pl.multiple_of(n * 128, 128), 128)
            for r in range(CAP):
                result[pl.ds(r * PEERS + g * GSIZE, GSIZE), cols] = scr[
                    pl.ds(r * PIECES + n, GSIZE, stride=PITCH), :
                ].astype(BF16)
            return carry

        lax.fori_loop(0, PIECES, line_up_back, 0)

    def combine(n, carry):
        cols = pl.ds(pl.multiple_of(n * 512, 512), 512)
        mout[:, cols] = jnp.dot(weights[...], result[:, cols], preferred_element_type=F32).astype(BF16)
        return carry

    lax.fori_loop(0, 4, combine, 0)
    store_moe = pltpu.make_async_copy(mout, moe_out_hbm, out_sem.at[1])
    store_moe.start()
    sent = sbuf.at[pl.ds(0, PEERS - 1)]
    pltpu.make_async_copy(sent, sent, d_send).wait()
    pltpu.make_async_copy(sent, sent, r_send).wait()
    w_wait(w_send.at[0], 6)
    w_wait(w_send.at[1], 18)
    w_wait(w_send.at[2], 24)
    store_mixed.wait()
    store_moe.wait()


def copy_out(mixed_in, moe_in, mixed_out, moe_out, mixed, moe, sem_in, sem_out):
    pieces = []
    for n in range(8):
        at = pl.ds(n * 128, 128)
        pieces.append((mixed_in.at[at, :], mixed.at[at, :], mixed_out.at[at, :]))
    pieces.append((moe_in, moe, moe_out))
    reads = [pltpu.make_async_copy(a, b, sem_in.at[n]) for n, (a, b, _) in enumerate(pieces)]
    writes = [pltpu.make_async_copy(b, o, sem_out.at[n]) for n, (_, b, o) in enumerate(pieces)]
    for read in reads:
        read.start()
    for read, write in zip(reads, writes):
        read.wait()
        write.start()
    for write in writes:
        write.wait()


def body(
    glu_value, glu_gate, conv_taps, chan_gain, chan_shift, mix_out_weight, moe_input, moe_gain, expert_ids,
    expert_share, expert_gate_weight, expert_up_weight, expert_down_weight,
):
    hbm = pl.BlockSpec(memory_space=pl.ANY)
    dma = pltpu.SemaphoreType.DMA
    mixed, moe_output = pl.pallas_call(
        kernel,
        out_shape=(
            jax.ShapeDtypeStruct((1024, 2048), BF16),
            jax.ShapeDtypeStruct((128, 2048), BF16),
        ),
        in_specs=[hbm] * 13,
        out_specs=(hbm, hbm),
        scratch_shapes=[
            pltpu.VMEM((31, 1024), F32),
            pltpu.VMEM((1, 1024), F32),
            pltpu.VMEM((1, 1024), F32),
            pltpu.VMEM((1, 2048), F32),
            pltpu.VMEM((4, 128), jnp.int32),
            pltpu.VMEM((4, 128), F32),
            pltpu.VMEM((1024, 1024), BF16),
            pltpu.VMEM((1024, 1024), BF16),
            pltpu.VMEM((2, HALO, 1024), BF16),
            pltpu.VMEM((8, 1024 + HALO + 8, 128), F32),
            pltpu.VMEM((8, 8 * SEGMENT, 128), F32),
            pltpu.VMEM((1024, 1024), BF16),
            pltpu.VMEM((8, 1024, 256), BF16),
            pltpu.VMEM((1024, 2048), BF16),
            pltpu.VMEM((128, 2048), BF16),
            pltpu.VMEM((128, 2048), BF16),
            pltpu.VMEM((128, PEERS), F32),
            pltpu.VMEM((128, PEERS), F32),
            pltpu.VMEM((PEERS, BLOCK, 128), BF16),
            pltpu.VMEM((PEERS, BLOCK, 128), BF16),
            pltpu.VMEM((PEERS, BLOCK, 128), BF16),
            pltpu.VMEM((PEERS, BLOCK, 128), BF16),
            pltpu.VMEM((GSIZE * PITCH, 128), F32),
            pltpu.VMEM((GSIZE * CAP, 2048), BF16),
            pltpu.VMEM((GSIZE * CAP, 1024), BF16),
            pltpu.VMEM((2048, 1024), BF16),
            pltpu.VMEM((2048, 1024), BF16),
            pltpu.VMEM((1024, 2048), BF16),
            pltpu.VMEM((PEERS * CAP, 2048), BF16),
            pltpu.VMEM((128, CAP * PEERS), BF16),
            pltpu.VMEM((128, 2048), BF16),
            dma((21,)), dma((2,)), dma((2,)), dma((2,)), dma((3,)), dma((3,)), dma, dma,
            dma, dma((GROUPS,)), dma, dma((GROUPS,)), dma((2,)),
        ],
        compiler_params=pltpu.CompilerParams(
            collective_id=0, has_side_effects=True, vmem_limit_bytes=62 * 2**20
        ),
        name="mixer",
    )(
        glu_value, glu_gate, conv_taps, chan_gain.reshape(1, -1), chan_shift.reshape(1, -1), mix_out_weight,
        moe_input, moe_gain.reshape(1, -1), expert_ids.T, expert_share.T,
        expert_gate_weight, expert_up_weight, expert_down_weight,
    )
    shapes = (mixed.shape, moe_output.shape)
    return pl.pallas_call(
        copy_out,
        out_shape=tuple(jax.ShapeDtypeStruct(shape, BF16) for shape in shapes),
        in_specs=[pl.BlockSpec(memory_space=pltpu.HBM)] * 2,
        out_specs=(pl.BlockSpec(memory_space=pltpu.HBM),) * 2,
        scratch_shapes=[*(pltpu.VMEM(shape, BF16) for shape in shapes), dma((9,)), dma((9,))],
        compiler_params=pltpu.CompilerParams(vmem_limit_bytes=63 * 2**20),
        name="copy_out",
    )(mixed, moe_output)


def solution(mesh):
    both = ("ep", "tp")
    placed = (
        P(both, None), P(both, None), P(), P(), P(), P("tp", None), P(both, None), P(), P(both, None),
        P(both, None), P(both, None, None), P(both, None, None), P(both, None, None),
    )
    return jax.shard_map(
        body,
        mesh=mesh,
        in_specs=placed,
        out_specs=(P(both, None), P(both, None)),
        check_vma=False,
    )
```

```python
import jax
import jax.numpy as jnp
import numpy as np
from jax import lax
from jax.experimental import pallas as pl
from jax.experimental.pallas import tpu as pltpu
from jax.sharding import PartitionSpec as P

MESH = pl.DeviceIdType.MESH
F32 = jnp.float32
BF16 = jnp.bfloat16
CLAMP_LIMIT = 7.0
GLU_SLOPE = 1.702
CAP = 5
PEERS = 128
GROUPS = 4
GSIZE = PEERS // GROUPS
PIECES = 16
BLOCK = CAP * PIECES
PITCH = 88
HALO = 32
SEGMENT = 129
CONV_STEP = 12
EARLY = 3
BORDER = 3
CONV_BLOCKS = -(-SEGMENT // CONV_STEP)


def sigmoid(v):
    return 0.5 + 0.5 * jnp.tanh(0.5 * v)


CLASSES = (
    ("220", "210", "120", "110", "200", "020", "100", "010", "000"),
    ("222", "212", "122", "221", "211", "121", "202"),
    ("022", "112", "111", "102", "002"),
    ("012", "201", "021", "101", "011", "001"),
)
SELF = 31


def steps(pattern, k):
    out, bit = [], 1
    for axis in pattern:
        if axis == "1":
            out.append(1 + 2 * ((k >> bit) & 1))
            bit += 1
        else:
            out.append(int(axis))
    return (*out, 1 - (k & 1))


def loops():
    groups, first = [], 0
    for patterns in CLASSES:
        groups.append([])
        for pattern in patterns:
            count = 2 << pattern.count("1")
            groups[-1].append((first, count, pattern))
            first += count
        assert first == GSIZE * len(groups)
    return groups


def places():
    flat = []
    for first, count, pattern in sum(loops(), []):
        for k in range(count):
            dz, dx, dy, dc = steps(pattern, k)
            flat.append(dz * 32 + dx * 8 + dy * 2 + dc)
    assert sorted(flat) == list(range(PEERS)) and flat[SELF] == 0
    return np.repeat(np.array(flat, np.int32)[:, None], 128, axis=1)


def kernel(
    value_hbm, gate_hbm, taps_hbm, cgain_hbm, cshift_hbm, wout_hbm, moe_hbm, mgain_hbm, ids_hbm, share_hbm, place_hbm,
    wg_hbm, wu_hbm, wd_hbm,
    mixed_hbm, moe_out_hbm,
    taps_ref, cgain_ref, cshift_ref, mgain_ref, ids_ref, share_ref, place_ref, value, gate, halo, glu, conv, act, wfull, obuf,
    xin, xn, rankm, sharem, sbuf, abuf, rbuf, tbuf, scr, rows, hidden, wg, wu, wd, result, weights, acc, mout,
    local_sem, out_sem, halo_send, halo_recv, w_send, w_recv, own_send, own_recv,
    d_send, d_recv, r_send, r_recv, self_sem,
):
    ep = lax.axis_index("ep")
    tp = lax.axis_index("tp")
    me = ep * 8 + tp
    z, x, y, c = ep >> 2, ep & 3, tp >> 1, tp & 1

    def device(dz, dx, dy, dc):
        return ((z + dz) & 3) * 4 + ((x + dx) & 3), ((y + dy) & 3) * 2 + ((c + dc) & 1)

    shard = pl.ds(pl.multiple_of(tp * 128, 128), 128)
    pairs = (
        (ids_hbm, ids_ref), (share_hbm, share_ref), (place_hbm, place_ref), (mgain_hbm, mgain_ref),
        (taps_hbm, taps_ref), (cgain_hbm, cgain_ref), (cshift_hbm, cshift_ref),
    )
    small = [pltpu.make_async_copy(a, b, local_sem.at[15 + n]) for n, (a, b) in enumerate(pairs)]
    load_moe = pltpu.make_async_copy(moe_hbm, xin, local_sem.at[0])
    load_w = [
        pltpu.make_async_copy(wout_hbm.at[:, pl.ds(n * 256, 256)], wfull.at[n, shard, :], local_sem.at[7 + n])
        for n in range(8)
    ]
    load_value = pltpu.make_async_copy(value_hbm, value, local_sem.at[2])
    load_gate = pltpu.make_async_copy(gate_hbm, gate, local_sem.at[3])
    load_wg = pltpu.make_async_copy(wg_hbm.at[0], wg, local_sem.at[4])
    load_wu = pltpu.make_async_copy(wu_hbm.at[0], wu, local_sem.at[5])
    load_wd = pltpu.make_async_copy(wd_hbm.at[0], wd, local_sem.at[6])
    for load in (*small[:4], load_moe):
        load.start()

    barrier = pltpu.get_barrier_semaphore()

    def hello(i, carry):
        target = me ^ i
        pl.semaphore_signal(barrier, inc=1, device_id=(target >> 3, target & 7), device_id_type=MESH)
        return carry

    lax.fori_loop(1, PEERS, hello, 0, unroll=3)

    for load in (*load_w, load_value, load_gate, *small[4:], load_wg, load_wu, load_wd):
        load.start()

    for load in small[:4]:
        load.wait()

    lane = lax.broadcasted_iota(jnp.int32, (PEERS, 128), 1)
    row = lax.broadcasted_iota(jnp.int32, (PEERS, 128), 0)
    j = place_ref[...]
    expert = (
        (((z + (j >> 5)) & 3) * 32) + (((x + (j >> 3)) & 3) * 8) + (((y + (j >> 1)) & 3) * 2) + ((c + j) & 1)
    )
    chosen = jnp.zeros((PEERS, 128), F32)
    shares = jnp.zeros((PEERS, 128), F32)
    for k in range(4):
        hit = ids_ref[k : k + 1, :] == expert
        chosen = jnp.where(hit, 1.0, chosen)
        shares = jnp.where(hit, share_ref[k : k + 1, :], shares)
    before = jnp.where(row < lane, 1.0, 0.0).astype(BF16)
    rank = jnp.dot(chosen.astype(BF16), before, preferred_element_type=F32)
    rankm[...] = jnp.where(chosen > 0.5, rank, -1.0)
    sharem[...] = shares

    load_moe.wait()

    def norm_rows(b, carry):
        at = pl.ds(pl.multiple_of(b * 32, 32), 32)
        f = xin[at, :].astype(F32)
        scaled = f * lax.rsqrt(jnp.mean(f * f, axis=-1, keepdims=True) + 1e-06)
        xn[at, :] = (scaled * mgain_ref[...]).astype(BF16)
        return carry

    lax.fori_loop(0, 4, norm_rows, 0)

    def pack(dst, first):
        def one(i, carry):
            dst[first + i] = scr[pl.ds(pl.multiple_of(i * PITCH, 8), BLOCK), :].astype(BF16)
            return carry

        lax.fori_loop(0, GSIZE, one, 0, unroll=4)

    def unpack(src, first):
        def one(i, carry):
            scr[pl.ds(pl.multiple_of(i * PITCH, 8), BLOCK), :] = src[first + i].astype(F32)
            return carry

        lax.fori_loop(0, GSIZE, one, 0, unroll=4)

    def spread(got, first):
        for r in range(CAP):
            for q in range(4):
                scr[pl.ds(r * PIECES + first + q, GSIZE, stride=PITCH), :] = got[
                    r * GSIZE : (r + 1) * GSIZE, q * 128 : (q + 1) * 128
                ]

    def gather(g, carry):
        ranks = rankm[pl.ds(pl.multiple_of(g * GSIZE, GSIZE), GSIZE), :]
        take = jnp.concatenate([jnp.where(ranks == float(r), 1.0, 0.0) for r in range(CAP)], axis=0).astype(BF16)
        for n in range(4):
            spread(jnp.dot(take, xn[:, n * 512 : (n + 1) * 512], preferred_element_type=F32), n * 4)
        pack(sbuf, g * GSIZE)
        return carry

    lax.fori_loop(0, GROUPS, gather, 0)
    load_value.wait()
    load_gate.wait()
    for load in load_w:
        load.wait()
    pl.semaphore_wait(barrier, PEERS - 1)

    nxt = (me + 1) & 127
    halo_copies = []
    for n, half in enumerate((value, gate)):
        cp = pltpu.make_async_remote_copy(
            src_ref=half.at[pl.ds(1024 - HALO, HALO), :], dst_ref=halo.at[n],
            send_sem=halo_send.at[n], recv_sem=halo_recv.at[n],
            device_id=(nxt >> 3, nxt & 7), device_id_type=MESH,
        )
        cp.start()
        halo_copies.append(cp)

    def w_block(n, rows_at, stage, target):
        pltpu.make_async_remote_copy(
            src_ref=wfull.at[n, rows_at, :], dst_ref=wfull.at[n, rows_at, :],
            send_sem=w_send.at[stage], recv_sem=w_recv.at[stage], device_id=target, device_id_type=MESH,
        ).start()

    def w_wait(sem, blocks):
        some = act.at[pl.ds(0, 32 * blocks), :]
        pltpu.make_async_copy(some, some, sem).wait()

    def origin(d):
        return pl.ds(pl.multiple_of((((y - d) & 3) * 2 + c) * 128, 128), 128)

    for d in range(1, 4):
        w_block(x, shard, 0, device(0, 0, d, 0))
        w_block(4 + z, shard, 0, device(0, 0, d, 0))
    own_forward = pltpu.make_async_remote_copy(
        src_ref=wfull.at[:, shard, :], dst_ref=wfull.at[:, shard, :], send_sem=own_send, recv_sem=own_recv,
        device_id=device(0, 0, 0, 1), device_id_type=MESH,
    )
    own_forward.start()

    self_copy = pltpu.make_async_copy(sbuf.at[SELF], abuf.at[SELF], self_sem.at[0])
    self_copy.start()

    sends = loops()

    def each(g, act_on):
        for first, count, pattern in sends[g]:

            def one(k, carry, first=first, pattern=pattern):
                act_on(first + k, steps(pattern, k))
                return carry

            lax.fori_loop(0, count - (pattern == "000"), one, 0)

    def send_group(g):
        def send(i, d):
            pltpu.make_async_remote_copy(
                src_ref=sbuf.at[i], dst_ref=abuf.at[i], send_sem=d_send, recv_sem=d_recv.at[g],
                device_id=device(*d), device_id_type=MESH,
            ).start()

        each(g, send)

    send_group(0)

    def glu_rows(b, carry):
        at = pl.ds(pl.multiple_of(b * 32, 32), 32)
        to = pl.ds(pl.multiple_of(b * 32 + HALO, 32), 32)
        gated = value[at, :].astype(F32) * sigmoid(gate[at, :].astype(F32))
        for l in range(8):
            glu[l, to, :] = gated[:, l * 128 : (l + 1) * 128]
        return carry

    lax.fori_loop(0, 1024 // 32, glu_rows, 0)
    for g in range(1, GROUPS):
        send_group(g)
    for l in range(8):
        glu[l, pl.ds(1024 + HALO, 8), :] = jnp.zeros((8, 128), F32)

    def conv_block(l, block):
        lanes = pl.ds(pl.multiple_of(l * 128, 128), 128)
        b0 = jnp.minimum(block * CONV_STEP, SEGMENT - CONV_STEP)
        near = [glu[l, pl.ds(b0 + 2 + u, 8, stride=SEGMENT), :] for u in range(CONV_STEP + 30)]
        totals = [None] * CONV_STEP
        for tap in range(31):
            w = jnp.broadcast_to(taps_ref[tap : tap + 1, lanes], (8, 128))
            for b in range(CONV_STEP):
                term = w * near[b + tap]
                totals[b] = term if tap == 0 else totals[b] + term
        for b in range(CONV_STEP):
            conv[l, pl.ds(b0 + b, 8, stride=SEGMENT), :] = totals[b]

    def conv_blocks(first, last):
        def one(n, carry):
            conv_block(n & 7, first + (n >> 3))
            return carry

        lax.fori_loop(0, 8 * (last - first), one, 0)

    for load in small[4:]:
        load.wait()
    conv_blocks(BORDER, BORDER + EARLY)

    for cp in halo_copies:
        cp.wait()
    border = halo[0].astype(F32) * sigmoid(halo[1].astype(F32))
    border = border * jnp.minimum(me, 1).astype(F32)
    for l in range(8):
        glu[l, pl.ds(0, HALO), :] = border[:, l * 128 : (l + 1) * 128]
    conv_blocks(0, BORDER)
    conv_blocks(BORDER + EARLY, CONV_BLOCKS)

    def norm_conv(n, carry):
        at = pl.ds(pl.multiple_of(n * 32, 32), 32)
        v = jnp.concatenate([conv[l, at, :] for l in range(8)], axis=-1)
        center = jnp.mean(v, axis=-1, keepdims=True)
        v = v - center
        spread = jnp.mean(v * v, axis=-1, keepdims=True)
        u = v * lax.rsqrt(spread + 1e-05) * cgain_ref[...] + cshift_ref[...]
        act[at, :] = (u * sigmoid(u)).astype(BF16)
        return carry

    lax.fori_loop(0, 32, norm_conv, 0, unroll=2)

    load_wg.wait()
    load_wu.wait()
    load_wd.wait()

    def group_wait(buf, sem, g):
        n = GSIZE - 1 if g == 0 else GSIZE
        pltpu.make_async_copy(buf.at[pl.ds(0, n)], buf.at[pl.ds(0, n)], sem.at[g]).wait()

    def experts(g):
        unpack(abuf, g * GSIZE)

        def line_up(n, carry):
            cols = pl.ds(pl.multiple_of(n * 128, 128), 128)
            for r in range(CAP):
                rows[pl.ds(r * GSIZE, GSIZE), cols] = scr[pl.ds(r * PIECES + n, GSIZE, stride=PITCH), :].astype(BF16)
            return carry

        lax.fori_loop(0, PIECES, line_up, 0)

        def up(n, carry):
            cols = pl.ds(pl.multiple_of(n * 512, 512), 512)
            pre_gate = jnp.dot(rows[...], wg[:, cols], preferred_element_type=F32)
            pre_up = jnp.dot(rows[...], wu[:, cols], preferred_element_type=F32)
            gated = jnp.minimum(pre_gate, CLAMP_LIMIT)
            lifted = jnp.clip(pre_up, -CLAMP_LIMIT, CLAMP_LIMIT) + 1.0
            hidden[:, cols] = (lifted * gated * sigmoid(GLU_SLOPE * gated)).astype(BF16)
            return carry

        lax.fori_loop(0, 2, up, 0)

        def down(n, carry):
            cols = pl.ds(pl.multiple_of(n * 512, 512), 512)
            spread(jnp.dot(hidden[...], wd[:, cols], preferred_element_type=F32), n * 4)
            return carry

        lax.fori_loop(0, 4, down, 0)
        pack(rbuf, g * GSIZE)

        def give_back(i, d):
            dz, dx, dy, dc = d
            pltpu.make_async_remote_copy(
                src_ref=rbuf.at[i], dst_ref=tbuf.at[i], send_sem=r_send, recv_sem=r_recv.at[g],
                device_id=device(-dz, -dx, -dy, dc), device_id_type=MESH,
            ).start()

        each(g, give_back)

    w_wait(w_recv.at[0], 6)
    for d in range(1, 4):
        for e in range(1, 4):
            w_block(x, origin(d), 1, device(0, e, 0, 0))
            w_block(4 + z, origin(d), 1, device(e, 0, 0, 0))

    self_copy.wait()
    group_wait(abuf, d_recv, 0)
    experts(0)
    self_back = pltpu.make_async_copy(rbuf.at[SELF], tbuf.at[SELF], self_sem.at[1])
    self_back.start()

    for g in range(1, GROUPS):
        group_wait(abuf, d_recv, g)
        experts(g)

    for g in range(GROUPS):
        ranks = rankm[g * GSIZE : (g + 1) * GSIZE, :]
        parts = sharem[g * GSIZE : (g + 1) * GSIZE, :]
        stacked = jnp.concatenate([jnp.where(ranks == float(r), parts, 0.0) for r in range(CAP)], axis=0)
        weights[pl.ds(g * GSIZE * CAP, GSIZE * CAP), :] = stacked.astype(BF16)

    w_wait(w_recv.at[1], 18)
    for d in range(1, 4):
        pltpu.make_async_remote_copy(
            src_ref=wfull.at[:, origin(d), :], dst_ref=wfull.at[:, origin(d), :],
            send_sem=w_send.at[2], recv_sem=w_recv.at[2], device_id=device(0, 0, 0, 1), device_id_type=MESH,
        ).start()
    own_forward.wait()
    w_wait(w_recv.at[2], 24)

    def project(n, carry):
        cols = pl.ds(pl.multiple_of(n * 256, 256), 256)
        for m in range(2):
            at = pl.ds(m * 512, 512)
            obuf[at, cols] = jnp.dot(act[at, :], wfull[n], preferred_element_type=F32).astype(BF16)
        return carry

    lax.fori_loop(0, 8, project, 0)

    store_mixed = pltpu.make_async_copy(obuf, mixed_hbm, out_sem.at[0])
    store_mixed.start()

    self_back.wait()

    def combine(first, n, last):
        at = pl.ds(first * GSIZE * CAP, (last - first) * GSIZE * CAP)
        cols = pl.ds(pl.multiple_of(n * 512, 512), 512)
        return lax.dot_general(
            weights[at, :], result[at, cols], (((0,), (0,)), ((), ())), preferred_element_type=F32
        ), cols

    for g in range(GROUPS):
        group_wait(tbuf, r_recv, g)
        unpack(tbuf, g * GSIZE)

        def line_up_back(n, carry, g=g):
            cols = pl.ds(pl.multiple_of(n * 128, 128), 128)
            for r in range(CAP):
                result[pl.ds((g * CAP + r) * GSIZE, GSIZE), cols] = scr[
                    pl.ds(r * PIECES + n, GSIZE, stride=PITCH), :
                ].astype(BF16)
            return carry

        lax.fori_loop(0, PIECES, line_up_back, 0)
        if g == GROUPS - 2:
            for n in range(4):
                got, cols = combine(0, n, GROUPS - 1)
                acc[:, cols] = got
    for n in range(4):
        got, cols = combine(GROUPS - 1, n, GROUPS)
        mout[:, cols] = (acc[:, cols] + got).astype(BF16)
    store_moe = pltpu.make_async_copy(mout, moe_out_hbm, out_sem.at[1])
    store_moe.start()
    sent = sbuf.at[pl.ds(0, PEERS - 1)]
    pltpu.make_async_copy(sent, sent, d_send).wait()
    pltpu.make_async_copy(sent, sent, r_send).wait()
    w_wait(w_send.at[0], 6)
    w_wait(w_send.at[1], 18)
    w_wait(w_send.at[2], 24)
    store_mixed.wait()
    store_moe.wait()


def copy_out(mixed_in, moe_in, mixed_out, moe_out, mixed, moe, sem_in, sem_out):
    pieces = []
    for n in range(8):
        at = pl.ds(n * 128, 128)
        pieces.append((mixed_in.at[at, :], mixed.at[at, :], mixed_out.at[at, :]))
    pieces.append((moe_in, moe, moe_out))
    reads = [pltpu.make_async_copy(a, b, sem_in.at[n]) for n, (a, b, _) in enumerate(pieces)]
    writes = [pltpu.make_async_copy(b, o, sem_out.at[n]) for n, (_, b, o) in enumerate(pieces)]
    for read in reads:
        read.start()
    for read, write in zip(reads, writes):
        read.wait()
        write.start()
    for write in writes:
        write.wait()


def body(
    glu_value, glu_gate, conv_taps, chan_gain, chan_shift, mix_out_weight, moe_input, moe_gain, expert_ids,
    expert_share, expert_gate_weight, expert_up_weight, expert_down_weight,
):
    hbm = pl.BlockSpec(memory_space=pl.ANY)
    dma = pltpu.SemaphoreType.DMA
    mixed, moe_output = pl.pallas_call(
        kernel,
        out_shape=(
            jax.ShapeDtypeStruct((1024, 2048), BF16),
            jax.ShapeDtypeStruct((128, 2048), BF16),
        ),
        in_specs=[hbm] * 14,
        out_specs=(hbm, hbm),
        scratch_shapes=[
            pltpu.VMEM((31, 1024), F32),
            pltpu.VMEM((1, 1024), F32),
            pltpu.VMEM((1, 1024), F32),
            pltpu.VMEM((1, 2048), F32),
            pltpu.VMEM((4, 128), jnp.int32),
            pltpu.VMEM((4, 128), F32),
            pltpu.VMEM((PEERS, 128), jnp.int32),
            pltpu.VMEM((1024, 1024), BF16),
            pltpu.VMEM((1024, 1024), BF16),
            pltpu.VMEM((2, HALO, 1024), BF16),
            pltpu.VMEM((8, 1024 + HALO + 8, 128), F32),
            pltpu.VMEM((8, 8 * SEGMENT, 128), F32),
            pltpu.VMEM((1024, 1024), BF16),
            pltpu.VMEM((8, 1024, 256), BF16),
            pltpu.VMEM((1024, 2048), BF16),
            pltpu.VMEM((128, 2048), BF16),
            pltpu.VMEM((128, 2048), BF16),
            pltpu.VMEM((128, PEERS), F32),
            pltpu.VMEM((128, PEERS), F32),
            pltpu.VMEM((PEERS, BLOCK, 128), BF16),
            pltpu.VMEM((PEERS, BLOCK, 128), BF16),
            pltpu.VMEM((PEERS, BLOCK, 128), BF16),
            pltpu.VMEM((PEERS, BLOCK, 128), BF16),
            pltpu.VMEM((GSIZE * PITCH, 128), F32),
            pltpu.VMEM((GSIZE * CAP, 2048), BF16),
            pltpu.VMEM((GSIZE * CAP, 1024), BF16),
            pltpu.VMEM((2048, 1024), BF16),
            pltpu.VMEM((2048, 1024), BF16),
            pltpu.VMEM((1024, 2048), BF16),
            pltpu.VMEM((PEERS * CAP, 2048), BF16),
            pltpu.VMEM((CAP * PEERS, 128), BF16),
            pltpu.VMEM((128, 2048), F32),
            pltpu.VMEM((128, 2048), BF16),
            dma((22,)), dma((2,)),  dma((2,)), dma((2,)), dma((3,)), dma((3,)), dma, dma,
            dma, dma((GROUPS,)), dma, dma((GROUPS,)), dma((2,)),
        ],
        compiler_params=pltpu.CompilerParams(
            collective_id=0, has_side_effects=True, vmem_limit_bytes=62 * 2**20
        ),
        name="mixer",
    )(
        glu_value, glu_gate, conv_taps, chan_gain.reshape(1, -1), chan_shift.reshape(1, -1), mix_out_weight,
        moe_input, moe_gain.reshape(1, -1), expert_ids.T, expert_share.T, places(),
        expert_gate_weight, expert_up_weight, expert_down_weight,
    )
    shapes = (mixed.shape, moe_output.shape)
    return pl.pallas_call(
        copy_out,
        out_shape=tuple(jax.ShapeDtypeStruct(shape, BF16) for shape in shapes),
        in_specs=[hbm, hbm],
        out_specs=(hbm, hbm),
        scratch_shapes=[*(pltpu.VMEM(shape, BF16) for shape in shapes), dma((9,)), dma((9,))],
        compiler_params=pltpu.CompilerParams(vmem_limit_bytes=63 * 2**20),
        name="copy_out",
    )(mixed, moe_output)


def solution(mesh):
    both = ("ep", "tp")
    placed = (
        P(both, None), P(both, None), P(), P(), P(), P("tp", None), P(both, None), P(), P(both, None),
        P(both, None), P(both, None, None), P(both, None, None), P(both, None, None),
    )
    return jax.shard_map(
        body,
        mesh=mesh,
        in_specs=placed,
        out_specs=(P(both, None), P(both, None)),
        check_vma=False,
    )
```

```python
import jax
import jax.numpy as jnp
import numpy as np
from jax import lax
from jax.experimental import pallas as pl
from jax.experimental.pallas import tpu as pltpu
from jax.sharding import PartitionSpec as P

MESH = pl.DeviceIdType.MESH
F32 = jnp.float32
BF16 = jnp.bfloat16
CLAMP_LIMIT = 7.0
GLU_SLOPE = 1.702
CAP = 5
PEERS = 128
GROUPS = 4
GSIZE = PEERS // GROUPS
PIECES = 16
BLOCK = CAP * PIECES
PITCH = 88
HALO = 32
SEGMENT = 129
CONV_STEP = 12
EARLY = 3
BORDER = 3
CONV_BLOCKS = -(-SEGMENT // CONV_STEP)


def sigmoid(v):
    return 0.5 + 0.5 * jnp.tanh(0.5 * v)


CLASSES = (
    ("220", "210", "120", "110", "200", "020", "100", "010", "000"),
    ("222", "212", "122", "221", "211", "121", "202"),
    ("022", "112", "111", "102", "002"),
    ("012", "201", "021", "101", "011", "001"),
)
SELF = 31


def steps(pattern, k):
    out, bit = [], 1
    for axis in pattern:
        if axis == "1":
            out.append(1 + 2 * ((k >> bit) & 1))
            bit += 1
        else:
            out.append(int(axis))
    return (*out, 1 - (k & 1))


def loops():
    groups, first = [], 0
    for patterns in CLASSES:
        groups.append([])
        for pattern in patterns:
            count = 2 << pattern.count("1")
            groups[-1].append((first, count, pattern))
            first += count
        assert first == GSIZE * len(groups)
    return groups


def places():
    flat = []
    for first, count, pattern in sum(loops(), []):
        for k in range(count):
            dz, dx, dy, dc = steps(pattern, k)
            flat.append(dz * 32 + dx * 8 + dy * 2 + dc)
    assert sorted(flat) == list(range(PEERS)) and flat[SELF] == 0
    return np.repeat(np.array(flat, np.int32)[:, None], 128, axis=1)


def kernel(
    value_hbm, gate_hbm, taps_hbm, cgain_hbm, cshift_hbm, wout_hbm, moe_hbm, mgain_hbm, ids_hbm, share_hbm, place_hbm,
    wg_hbm, wu_hbm, wd_hbm,
    mixed_hbm, moe_out_hbm,
    taps_ref, cgain_ref, cshift_ref, mgain_ref, ids_ref, share_ref, place_ref, value, gate, edge, halo, glu, conv, act, wfull, obuf,
    xin, xn, rankm, sharem, sbuf, abuf, rbuf, tbuf, scr, rows, hidden, wg, wu, wd, result, weights, acc, mout,
    local_sem, out_sem, halo_send, halo_recv, w_send, w_recv, own_send, own_recv,
    d_send, d_recv, r_send, r_recv, self_sem,
):
    ep = lax.axis_index("ep")
    tp = lax.axis_index("tp")
    me = ep * 8 + tp
    z, x, y, c = ep >> 2, ep & 3, tp >> 1, tp & 1

    def device(dz, dx, dy, dc):
        return ((z + dz) & 3) * 4 + ((x + dx) & 3), ((y + dy) & 3) * 2 + ((c + dc) & 1)

    shard = pl.ds(pl.multiple_of(tp * 128, 128), 128)
    pairs = (
        (ids_hbm, ids_ref), (share_hbm, share_ref), (place_hbm, place_ref), (mgain_hbm, mgain_ref),
        (taps_hbm, taps_ref), (cgain_hbm, cgain_ref), (cshift_hbm, cshift_ref),
    )
    small = [pltpu.make_async_copy(a, b, local_sem.at[15 + n]) for n, (a, b) in enumerate(pairs)]
    load_moe = pltpu.make_async_copy(moe_hbm, xin, local_sem.at[0])
    load_w = [
        pltpu.make_async_copy(wout_hbm.at[:, pl.ds(n * 256, 256)], wfull.at[n, shard, :], local_sem.at[7 + n])
        for n in range(8)
    ]
    load_value = pltpu.make_async_copy(value_hbm, value, local_sem.at[2])
    load_gate = pltpu.make_async_copy(gate_hbm, gate, local_sem.at[3])
    load_wg = pltpu.make_async_copy(wg_hbm.at[0], wg, local_sem.at[4])
    load_wu = pltpu.make_async_copy(wu_hbm.at[0], wu, local_sem.at[5])
    load_wd = pltpu.make_async_copy(wd_hbm.at[0], wd, local_sem.at[6])
    ends = pl.ds(1024 - HALO, HALO)
    load_ends = [
        pltpu.make_async_copy(half.at[ends, :], edge.at[n], local_sem.at[22 + n])
        for n, half in enumerate((value_hbm, gate_hbm))
    ]
    for load in (*small[:4], load_moe, *load_ends, *load_w):
        load.start()

    barrier = pltpu.get_barrier_semaphore()

    def hello(i, carry):
        target = me ^ (PEERS - 1 - i)
        pl.semaphore_signal(barrier, inc=1, device_id=(target >> 3, target & 7), device_id_type=MESH)
        return carry

    lax.fori_loop(0, PEERS - 1, hello, 0, unroll=3)

    for load in (load_value, load_gate, *small[4:], load_wg, load_wu, load_wd):
        load.start()

    for load in small[:4]:
        load.wait()

    lane = lax.broadcasted_iota(jnp.int32, (PEERS, 128), 1)
    row = lax.broadcasted_iota(jnp.int32, (PEERS, 128), 0)
    j = place_ref[...]
    expert = (
        (((z + (j >> 5)) & 3) * 32) + (((x + (j >> 3)) & 3) * 8) + (((y + (j >> 1)) & 3) * 2) + ((c + j) & 1)
    )
    chosen = jnp.zeros((PEERS, 128), F32)
    shares = jnp.zeros((PEERS, 128), F32)
    for k in range(4):
        hit = ids_ref[k : k + 1, :] == expert
        chosen = jnp.where(hit, 1.0, chosen)
        shares = jnp.where(hit, share_ref[k : k + 1, :], shares)
    before = jnp.where(row < lane, 1.0, 0.0).astype(BF16)
    rank = jnp.dot(chosen.astype(BF16), before, preferred_element_type=F32)
    rankm[...] = jnp.where(chosen > 0.5, rank, -1.0)
    sharem[...] = shares

    load_moe.wait()

    def norm_rows(b, carry):
        at = pl.ds(pl.multiple_of(b * 32, 32), 32)
        f = xin[at, :].astype(F32)
        scaled = f * lax.rsqrt(jnp.mean(f * f, axis=-1, keepdims=True) + 1e-06)
        xn[at, :] = (scaled * mgain_ref[...]).astype(BF16)
        return carry

    lax.fori_loop(0, 4, norm_rows, 0)

    def pack(dst, first):
        def one(i, carry):
            dst[first + i] = scr[pl.ds(pl.multiple_of(i * PITCH, 8), BLOCK), :].astype(BF16)
            return carry

        lax.fori_loop(0, GSIZE, one, 0, unroll=4)

    def unpack(src, first):
        def one(i, carry):
            scr[pl.ds(pl.multiple_of(i * PITCH, 8), BLOCK), :] = src[first + i].astype(F32)
            return carry

        lax.fori_loop(0, GSIZE, one, 0, unroll=4)

    def spread(got, first):
        for r in range(CAP):
            for q in range(4):
                scr[pl.ds(r * PIECES + first + q, GSIZE, stride=PITCH), :] = got[
                    r * GSIZE : (r + 1) * GSIZE, q * 128 : (q + 1) * 128
                ]

    def gather(g, carry):
        ranks = rankm[pl.ds(pl.multiple_of(g * GSIZE, GSIZE), GSIZE), :]
        take = jnp.concatenate([jnp.where(ranks == float(r), 1.0, 0.0) for r in range(CAP)], axis=0).astype(BF16)
        for n in range(4):
            spread(jnp.dot(take, xn[:, n * 512 : (n + 1) * 512], preferred_element_type=F32), n * 4)
        pack(sbuf, g * GSIZE)
        return carry

    gather(0, 0)
    for load in (*load_ends, *load_w):
        load.wait()
    pl.semaphore_wait(barrier, PEERS - 1)

    nxt = (me + 1) & 127
    halo_copies = []
    for n in range(2):
        cp = pltpu.make_async_remote_copy(
            src_ref=edge.at[n], dst_ref=halo.at[n],
            send_sem=halo_send.at[n], recv_sem=halo_recv.at[n],
            device_id=(nxt >> 3, nxt & 7), device_id_type=MESH,
        )
        cp.start()
        halo_copies.append(cp)

    def w_block(n, rows_at, stage, target):
        pltpu.make_async_remote_copy(
            src_ref=wfull.at[n, rows_at, :], dst_ref=wfull.at[n, rows_at, :],
            send_sem=w_send.at[stage], recv_sem=w_recv.at[stage], device_id=target, device_id_type=MESH,
        ).start()

    def w_wait(sem, blocks):
        some = act.at[pl.ds(0, 32 * blocks), :]
        pltpu.make_async_copy(some, some, sem).wait()

    def origin(d):
        return pl.ds(pl.multiple_of((((y - d) & 3) * 2 + c) * 128, 128), 128)

    for d in range(1, 4):
        w_block(x, shard, 0, device(0, 0, d, 0))
        w_block(4 + z, shard, 0, device(0, 0, d, 0))
    own_forward = pltpu.make_async_remote_copy(
        src_ref=wfull.at[:, shard, :], dst_ref=wfull.at[:, shard, :], send_sem=own_send, recv_sem=own_recv,
        device_id=device(0, 0, 0, 1), device_id_type=MESH,
    )
    own_forward.start()

    self_copy = pltpu.make_async_copy(sbuf.at[SELF], abuf.at[SELF], self_sem.at[0])
    self_copy.start()

    sends = loops()

    def each(g, act_on):
        for first, count, pattern in sends[g]:

            def one(k, carry, first=first, pattern=pattern):
                act_on(first + k, steps(pattern, k))
                return carry

            lax.fori_loop(0, count - (pattern == "000"), one, 0)

    def send_group(g):
        def send(i, d):
            pltpu.make_async_remote_copy(
                src_ref=sbuf.at[i], dst_ref=abuf.at[i], send_sem=d_send, recv_sem=d_recv.at[g],
                device_id=device(*d), device_id_type=MESH,
            ).start()

        each(g, send)

    send_group(0)
    lax.fori_loop(1, GROUPS, gather, 0)
    for g in range(1, GROUPS):
        send_group(g)

    load_value.wait()
    load_gate.wait()

    def glu_rows(b, carry):
        at = pl.ds(pl.multiple_of(b * 32, 32), 32)
        to = pl.ds(pl.multiple_of(b * 32 + HALO, 32), 32)
        gated = value[at, :].astype(F32) * sigmoid(gate[at, :].astype(F32))
        for l in range(8):
            glu[l, to, :] = gated[:, l * 128 : (l + 1) * 128]
        return carry

    lax.fori_loop(0, 1024 // 32, glu_rows, 0)
    for l in range(8):
        glu[l, pl.ds(1024 + HALO, 8), :] = jnp.zeros((8, 128), F32)

    def conv_block(l, block):
        lanes = pl.ds(pl.multiple_of(l * 128, 128), 128)
        b0 = jnp.minimum(block * CONV_STEP, SEGMENT - CONV_STEP)
        near = [glu[l, pl.ds(b0 + 2 + u, 8, stride=SEGMENT), :] for u in range(CONV_STEP + 30)]
        totals = [None] * CONV_STEP
        for tap in range(31):
            w = jnp.broadcast_to(taps_ref[tap : tap + 1, lanes], (8, 128))
            for b in range(CONV_STEP):
                term = w * near[b + tap]
                totals[b] = term if tap == 0 else totals[b] + term
        for b in range(CONV_STEP):
            conv[l, pl.ds(b0 + b, 8, stride=SEGMENT), :] = totals[b]

    def conv_blocks(first, last):
        def one(n, carry):
            conv_block(n & 7, first + (n >> 3))
            return carry

        lax.fori_loop(0, 8 * (last - first), one, 0)

    for load in small[4:]:
        load.wait()
    conv_blocks(BORDER, BORDER + EARLY)

    for cp in halo_copies:
        cp.wait()
    border = halo[0].astype(F32) * sigmoid(halo[1].astype(F32))
    border = border * jnp.minimum(me, 1).astype(F32)
    for l in range(8):
        glu[l, pl.ds(0, HALO), :] = border[:, l * 128 : (l + 1) * 128]
    conv_blocks(0, BORDER)
    conv_blocks(BORDER + EARLY, CONV_BLOCKS)

    def norm_conv(n, carry):
        at = pl.ds(pl.multiple_of(n * 32, 32), 32)
        v = jnp.concatenate([conv[l, at, :] for l in range(8)], axis=-1)
        center = jnp.mean(v, axis=-1, keepdims=True)
        v = v - center
        spread = jnp.mean(v * v, axis=-1, keepdims=True)
        u = v * lax.rsqrt(spread + 1e-05) * cgain_ref[...] + cshift_ref[...]
        act[at, :] = (u * sigmoid(u)).astype(BF16)
        return carry

    lax.fori_loop(0, 32, norm_conv, 0, unroll=2)

    load_wg.wait()
    load_wu.wait()
    load_wd.wait()

    def group_wait(buf, sem, g):
        n = GSIZE - 1 if g == 0 else GSIZE
        pltpu.make_async_copy(buf.at[pl.ds(0, n)], buf.at[pl.ds(0, n)], sem.at[g]).wait()

    def experts(g):
        unpack(abuf, g * GSIZE)

        def line_up(n, carry):
            cols = pl.ds(pl.multiple_of(n * 128, 128), 128)
            for r in range(CAP):
                rows[pl.ds(r * GSIZE, GSIZE), cols] = scr[pl.ds(r * PIECES + n, GSIZE, stride=PITCH), :].astype(BF16)
            return carry

        lax.fori_loop(0, PIECES, line_up, 0)

        def up(n, carry):
            cols = pl.ds(pl.multiple_of(n * 512, 512), 512)
            pre_gate = jnp.dot(rows[...], wg[:, cols], preferred_element_type=F32)
            pre_up = jnp.dot(rows[...], wu[:, cols], preferred_element_type=F32)
            gated = jnp.minimum(pre_gate, CLAMP_LIMIT)
            lifted = jnp.clip(pre_up, -CLAMP_LIMIT, CLAMP_LIMIT) + 1.0
            hidden[:, cols] = (lifted * gated * sigmoid(GLU_SLOPE * gated)).astype(BF16)
            return carry

        lax.fori_loop(0, 2, up, 0)

        def down(n, carry):
            cols = pl.ds(pl.multiple_of(n * 512, 512), 512)
            spread(jnp.dot(hidden[...], wd[:, cols], preferred_element_type=F32), n * 4)
            return carry

        lax.fori_loop(0, 4, down, 0)
        pack(rbuf, g * GSIZE)

        def give_back(i, d):
            dz, dx, dy, dc = d
            pltpu.make_async_remote_copy(
                src_ref=rbuf.at[i], dst_ref=tbuf.at[i], send_sem=r_send, recv_sem=r_recv.at[g],
                device_id=device(-dz, -dx, -dy, dc), device_id_type=MESH,
            ).start()

        each(g, give_back)

    w_wait(w_recv.at[0], 6)
    for d in range(1, 4):
        for e in range(1, 4):
            w_block(x, origin(d), 1, device(0, e, 0, 0))
            w_block(4 + z, origin(d), 1, device(e, 0, 0, 0))

    self_copy.wait()
    group_wait(abuf, d_recv, 0)
    experts(0)
    self_back = pltpu.make_async_copy(rbuf.at[SELF], tbuf.at[SELF], self_sem.at[1])
    self_back.start()

    for g in range(1, GROUPS):
        group_wait(abuf, d_recv, g)
        experts(g)

    for g in range(GROUPS):
        ranks = rankm[g * GSIZE : (g + 1) * GSIZE, :]
        parts = sharem[g * GSIZE : (g + 1) * GSIZE, :]
        stacked = jnp.concatenate([jnp.where(ranks == float(r), parts, 0.0) for r in range(CAP)], axis=0)
        weights[pl.ds(g * GSIZE * CAP, GSIZE * CAP), :] = stacked.astype(BF16)

    w_wait(w_recv.at[1], 18)
    for d in range(1, 4):
        pltpu.make_async_remote_copy(
            src_ref=wfull.at[:, origin(d), :], dst_ref=wfull.at[:, origin(d), :],
            send_sem=w_send.at[2], recv_sem=w_recv.at[2], device_id=device(0, 0, 0, 1), device_id_type=MESH,
        ).start()
    own_forward.wait()
    w_wait(w_recv.at[2], 24)

    def project(n, carry):
        cols = pl.ds(pl.multiple_of(n * 256, 256), 256)
        for m in range(2):
            at = pl.ds(m * 512, 512)
            obuf[at, cols] = jnp.dot(act[at, :], wfull[n], preferred_element_type=F32).astype(BF16)
        return carry

    lax.fori_loop(0, 8, project, 0)

    store_mixed = pltpu.make_async_copy(obuf, mixed_hbm, out_sem.at[0])
    store_mixed.start()

    self_back.wait()

    def combine(first, n, last):
        at = pl.ds(first * GSIZE * CAP, (last - first) * GSIZE * CAP)
        cols = pl.ds(pl.multiple_of(n * 512, 512), 512)
        return lax.dot_general(
            weights[at, :], result[at, cols], (((0,), (0,)), ((), ())), preferred_element_type=F32
        ), cols

    for g in range(GROUPS):
        group_wait(tbuf, r_recv, g)
        unpack(tbuf, g * GSIZE)

        def line_up_back(n, carry, g=g):
            cols = pl.ds(pl.multiple_of(n * 128, 128), 128)
            for r in range(CAP):
                result[pl.ds((g * CAP + r) * GSIZE, GSIZE), cols] = scr[
                    pl.ds(r * PIECES + n, GSIZE, stride=PITCH), :
                ].astype(BF16)
            return carry

        lax.fori_loop(0, PIECES, line_up_back, 0)
        if g == GROUPS - 2:
            for n in range(4):
                got, cols = combine(0, n, GROUPS - 1)
                acc[:, cols] = got
    for n in range(4):
        got, cols = combine(GROUPS - 1, n, GROUPS)
        mout[:, cols] = (acc[:, cols] + got).astype(BF16)
    store_moe = pltpu.make_async_copy(mout, moe_out_hbm, out_sem.at[1])
    store_moe.start()
    sent = sbuf.at[pl.ds(0, PEERS - 1)]
    pltpu.make_async_copy(sent, sent, d_send).wait()
    pltpu.make_async_copy(sent, sent, r_send).wait()
    w_wait(w_send.at[0], 6)
    w_wait(w_send.at[1], 18)
    w_wait(w_send.at[2], 24)
    store_mixed.wait()
    store_moe.wait()


def copy_out(mixed_in, moe_in, mixed_out, moe_out, mixed, moe, sem_in, sem_out):
    pieces = []
    for n in range(4):
        at = pl.ds(n * 256, 256)
        pieces.append((mixed_in.at[at, :], mixed.at[at, :], mixed_out.at[at, :]))
    pieces.append((moe_in, moe, moe_out))
    reads = [pltpu.make_async_copy(a, b, sem_in.at[n]) for n, (a, b, _) in enumerate(pieces)]
    writes = [pltpu.make_async_copy(b, o, sem_out.at[n]) for n, (_, b, o) in enumerate(pieces)]
    for read in reads:
        read.start()
    for read, write in zip(reads, writes):
        read.wait()
        write.start()
    for write in writes:
        write.wait()


def body(
    glu_value, glu_gate, conv_taps, chan_gain, chan_shift, mix_out_weight, moe_input, moe_gain, expert_ids,
    expert_share, expert_gate_weight, expert_up_weight, expert_down_weight,
):
    hbm = pl.BlockSpec(memory_space=pl.ANY)
    dma = pltpu.SemaphoreType.DMA
    mixed, moe_output = pl.pallas_call(
        kernel,
        out_shape=(
            jax.ShapeDtypeStruct((1024, 2048), BF16),
            jax.ShapeDtypeStruct((128, 2048), BF16),
        ),
        in_specs=[hbm] * 14,
        out_specs=(hbm, hbm),
        scratch_shapes=[
            pltpu.VMEM((31, 1024), F32),
            pltpu.VMEM((1, 1024), F32),
            pltpu.VMEM((1, 1024), F32),
            pltpu.VMEM((1, 2048), F32),
            pltpu.VMEM((4, 128), jnp.int32),
            pltpu.VMEM((4, 128), F32),
            pltpu.VMEM((PEERS, 128), jnp.int32),
            pltpu.VMEM((1024, 1024), BF16),
            pltpu.VMEM((1024, 1024), BF16),
            pltpu.VMEM((2, HALO, 1024), BF16),
            pltpu.VMEM((2, HALO, 1024), BF16),
            pltpu.VMEM((8, 1024 + HALO + 8, 128), F32),
            pltpu.VMEM((8, 8 * SEGMENT, 128), F32),
            pltpu.VMEM((1024, 1024), BF16),
            pltpu.VMEM((8, 1024, 256), BF16),
            pltpu.VMEM((1024, 2048), BF16),
            pltpu.VMEM((128, 2048), BF16),
            pltpu.VMEM((128, 2048), BF16),
            pltpu.VMEM((128, PEERS), F32),
            pltpu.VMEM((128, PEERS), F32),
            pltpu.VMEM((PEERS, BLOCK, 128), BF16),
            pltpu.VMEM((PEERS, BLOCK, 128), BF16),
            pltpu.VMEM((PEERS, BLOCK, 128), BF16),
            pltpu.VMEM((PEERS, BLOCK, 128), BF16),
            pltpu.VMEM((GSIZE * PITCH, 128), F32),
            pltpu.VMEM((GSIZE * CAP, 2048), BF16),
            pltpu.VMEM((GSIZE * CAP, 1024), BF16),
            pltpu.VMEM((2048, 1024), BF16),
            pltpu.VMEM((2048, 1024), BF16),
            pltpu.VMEM((1024, 2048), BF16),
            pltpu.VMEM((PEERS * CAP, 2048), BF16),
            pltpu.VMEM((CAP * PEERS, 128), BF16),
            pltpu.VMEM((128, 2048), F32),
            pltpu.VMEM((128, 2048), BF16),
            dma((24,)), dma((2,)),  dma((2,)), dma((2,)), dma((3,)), dma((3,)), dma, dma,
            dma, dma((GROUPS,)), dma, dma((GROUPS,)), dma((2,)),
        ],
        compiler_params=pltpu.CompilerParams(
            collective_id=0, has_side_effects=True, vmem_limit_bytes=62 * 2**20
        ),
        name="mixer",
    )(
        glu_value, glu_gate, conv_taps, chan_gain.reshape(1, -1), chan_shift.reshape(1, -1), mix_out_weight,
        moe_input, moe_gain.reshape(1, -1), expert_ids.T, expert_share.T, places(),
        expert_gate_weight, expert_up_weight, expert_down_weight,
    )
    shapes = (mixed.shape, moe_output.shape)
    return pl.pallas_call(
        copy_out,
        out_shape=tuple(jax.ShapeDtypeStruct(shape, BF16) for shape in shapes),
        in_specs=[hbm, hbm],
        out_specs=(hbm, hbm),
        scratch_shapes=[*(pltpu.VMEM(shape, BF16) for shape in shapes), dma((5,)), dma((5,))],
        compiler_params=pltpu.CompilerParams(vmem_limit_bytes=63 * 2**20),
        name="copy_out",
    )(mixed, moe_output)


def solution(mesh):
    both = ("ep", "tp")
    placed = (
        P(both, None), P(both, None), P(), P(), P(), P("tp", None), P(both, None), P(), P(both, None),
        P(both, None), P(both, None, None), P(both, None, None), P(both, None, None),
    )
    return jax.shard_map(
        body,
        mesh=mesh,
        in_specs=placed,
        out_specs=(P(both, None), P(both, None)),
        check_vma=False,
    )
```

```python
import jax
import jax.numpy as jnp
import numpy as np
from jax import lax
from jax.experimental import pallas as pl
from jax.experimental.pallas import tpu as pltpu
from jax.sharding import PartitionSpec as P

MESH = pl.DeviceIdType.MESH
F32 = jnp.float32
BF16 = jnp.bfloat16
CLAMP_LIMIT = 7.0
GLU_SLOPE = 1.702
CAP = 5
PEERS = 128
GROUPS = 4
GSIZE = PEERS // GROUPS
PIECES = 16
BLOCK = CAP * PIECES
PITCH = 88
HALO = 32
SEGMENT = 129
CONV_STEP = 12
EARLY = 3
BORDER = 3
CONV_BLOCKS = -(-SEGMENT // CONV_STEP)


def sigmoid(v):
    return 0.5 + 0.5 * jnp.tanh(0.5 * v)


CLASSES = (
    ("220", "210", "120", "110", "200", "020", "100", "010", "000"),
    ("222", "212", "122", "221", "211", "121", "202"),
    ("022", "112", "111", "102", "002"),
    ("012", "201", "021", "101", "011", "001"),
)
SELF = 31
LAST = (PEERS - GSIZE) * CAP


def weighted(weights, rows):
    return lax.dot_general(weights, rows, (((0,), (0,)), ((), ())), preferred_element_type=F32)


def steps(pattern, k):
    out, bit = [], 1
    for axis in pattern:
        if axis == "1":
            out.append(1 + 2 * ((k >> bit) & 1))
            bit += 1
        else:
            out.append(int(axis))
    return (*out, 1 - (k & 1))


def loops():
    groups, first = [], 0
    for patterns in CLASSES:
        groups.append([])
        for pattern in patterns:
            count = 2 << pattern.count("1")
            groups[-1].append((first, count, pattern))
            first += count
        assert first == GSIZE * len(groups)
    return groups


def places():
    flat = []
    for first, count, pattern in sum(loops(), []):
        for k in range(count):
            dz, dx, dy, dc = steps(pattern, k)
            flat.append(dz * 32 + dx * 8 + dy * 2 + dc)
    assert sorted(flat) == list(range(PEERS)) and flat[SELF] == 0
    return np.repeat(np.array(flat, np.int32)[:, None], 128, axis=1)


def kernel(
    value_hbm, gate_hbm, taps_hbm, cgain_hbm, cshift_hbm, wout_hbm, moe_hbm, mgain_hbm, ids_hbm, share_hbm, place_hbm,
    wg_hbm, wu_hbm, wd_hbm,
    mixed_hbm, acc_hbm, last_weights_hbm, last_hbm,
    taps_ref, cgain_ref, cshift_ref, mgain_ref, ids_ref, share_ref, place_ref, value, gate, edge, halo, glu, conv, act, wfull, obuf,
    xin, xn, rankm, sharem, sbuf, abuf, rbuf, tbuf, scr, rows, hidden, wg, wu, wd, result, weights, acc,
    local_sem, out_sem, halo_send, halo_recv, w_send, w_recv, own_send, own_recv,
    d_send, d_recv, r_send, r_recv, self_sem,
):
    ep = lax.axis_index("ep")
    tp = lax.axis_index("tp")
    me = ep * 8 + tp
    z, x, y, c = ep >> 2, ep & 3, tp >> 1, tp & 1

    def device(dz, dx, dy, dc):
        return ((z + dz) & 3) * 4 + ((x + dx) & 3), ((y + dy) & 3) * 2 + ((c + dc) & 1)

    shard = pl.ds(pl.multiple_of(tp * 128, 128), 128)
    pairs = (
        (ids_hbm, ids_ref), (share_hbm, share_ref), (place_hbm, place_ref), (mgain_hbm, mgain_ref),
        (taps_hbm, taps_ref), (cgain_hbm, cgain_ref), (cshift_hbm, cshift_ref),
    )
    small = [pltpu.make_async_copy(a, b, local_sem.at[15 + n]) for n, (a, b) in enumerate(pairs)]
    load_moe = pltpu.make_async_copy(moe_hbm, xin, local_sem.at[0])
    load_w = [
        pltpu.make_async_copy(wout_hbm.at[:, pl.ds(n * 256, 256)], wfull.at[n, shard, :], local_sem.at[7 + n])
        for n in range(8)
    ]
    load_value = pltpu.make_async_copy(value_hbm, value, local_sem.at[2])
    load_gate = pltpu.make_async_copy(gate_hbm, gate, local_sem.at[3])
    load_wg = pltpu.make_async_copy(wg_hbm.at[0], wg, local_sem.at[4])
    load_wu = pltpu.make_async_copy(wu_hbm.at[0], wu, local_sem.at[5])
    load_wd = pltpu.make_async_copy(wd_hbm.at[0], wd, local_sem.at[6])
    ends = pl.ds(1024 - HALO, HALO)
    load_ends = [
        pltpu.make_async_copy(half.at[ends, :], edge.at[n], local_sem.at[22 + n])
        for n, half in enumerate((value_hbm, gate_hbm))
    ]
    for load in (*small[:4], load_moe, *load_ends, *load_w):
        load.start()

    barrier = pltpu.get_barrier_semaphore()

    def hello(i, carry):
        target = me ^ (PEERS - 1 - i)
        pl.semaphore_signal(barrier, inc=1, device_id=(target >> 3, target & 7), device_id_type=MESH)
        return carry

    lax.fori_loop(0, PEERS - 1, hello, 0, unroll=3)

    for load in (load_value, load_gate, *small[4:], load_wg, load_wu, load_wd):
        load.start()

    for load in small[:4]:
        load.wait()

    lane = lax.broadcasted_iota(jnp.int32, (PEERS, 128), 1)
    row = lax.broadcasted_iota(jnp.int32, (PEERS, 128), 0)
    j = place_ref[...]
    expert = (
        (((z + (j >> 5)) & 3) * 32) + (((x + (j >> 3)) & 3) * 8) + (((y + (j >> 1)) & 3) * 2) + ((c + j) & 1)
    )
    chosen = jnp.zeros((PEERS, 128), F32)
    shares = jnp.zeros((PEERS, 128), F32)
    for k in range(4):
        hit = ids_ref[k : k + 1, :] == expert
        chosen = jnp.where(hit, 1.0, chosen)
        shares = jnp.where(hit, share_ref[k : k + 1, :], shares)
    before = jnp.where(row < lane, 1.0, 0.0).astype(BF16)
    rank = jnp.dot(chosen.astype(BF16), before, preferred_element_type=F32)
    rankm[...] = jnp.where(chosen > 0.5, rank, -1.0)
    sharem[...] = shares

    load_moe.wait()

    def norm_rows(b, carry):
        at = pl.ds(pl.multiple_of(b * 32, 32), 32)
        f = xin[at, :].astype(F32)
        scaled = f * lax.rsqrt(jnp.mean(f * f, axis=-1, keepdims=True) + 1e-06)
        xn[at, :] = (scaled * mgain_ref[...]).astype(BF16)
        return carry

    lax.fori_loop(0, 4, norm_rows, 0)

    def pack(dst, first):
        def one(i, carry):
            dst[first + i] = scr[pl.ds(pl.multiple_of(i * PITCH, 8), BLOCK), :].astype(BF16)
            return carry

        lax.fori_loop(0, GSIZE, one, 0, unroll=4)

    def unpack(src, first):
        def one(i, carry):
            scr[pl.ds(pl.multiple_of(i * PITCH, 8), BLOCK), :] = src[first + i].astype(F32)
            return carry

        lax.fori_loop(0, GSIZE, one, 0, unroll=4)

    def spread(got, first):
        for r in range(CAP):
            for q in range(4):
                scr[pl.ds(r * PIECES + first + q, GSIZE, stride=PITCH), :] = got[
                    r * GSIZE : (r + 1) * GSIZE, q * 128 : (q + 1) * 128
                ]

    def gather(g, carry):
        ranks = rankm[pl.ds(pl.multiple_of(g * GSIZE, GSIZE), GSIZE), :]
        take = jnp.concatenate([jnp.where(ranks == float(r), 1.0, 0.0) for r in range(CAP)], axis=0).astype(BF16)
        for n in range(4):
            spread(jnp.dot(take, xn[:, n * 512 : (n + 1) * 512], preferred_element_type=F32), n * 4)
        pack(sbuf, g * GSIZE)
        return carry

    gather(0, 0)
    for load in (*load_ends, *load_w):
        load.wait()
    pl.semaphore_wait(barrier, PEERS - 1)

    nxt = (me + 1) & 127
    halo_copies = []
    for n in range(2):
        cp = pltpu.make_async_remote_copy(
            src_ref=edge.at[n], dst_ref=halo.at[n],
            send_sem=halo_send.at[n], recv_sem=halo_recv.at[n],
            device_id=(nxt >> 3, nxt & 7), device_id_type=MESH,
        )
        cp.start()
        halo_copies.append(cp)

    def w_block(n, rows_at, stage, target):
        pltpu.make_async_remote_copy(
            src_ref=wfull.at[n, rows_at, :], dst_ref=wfull.at[n, rows_at, :],
            send_sem=w_send.at[stage], recv_sem=w_recv.at[stage], device_id=target, device_id_type=MESH,
        ).start()

    def w_wait(sem, blocks):
        some = act.at[pl.ds(0, 32 * blocks), :]
        pltpu.make_async_copy(some, some, sem).wait()

    def origin(d):
        return pl.ds(pl.multiple_of((((y - d) & 3) * 2 + c) * 128, 128), 128)

    for d in range(1, 4):
        w_block(x, shard, 0, device(0, 0, d, 0))
        w_block(4 + z, shard, 0, device(0, 0, d, 0))
    own_forward = pltpu.make_async_remote_copy(
        src_ref=wfull.at[:, shard, :], dst_ref=wfull.at[:, shard, :], send_sem=own_send, recv_sem=own_recv,
        device_id=device(0, 0, 0, 1), device_id_type=MESH,
    )
    own_forward.start()

    self_copy = pltpu.make_async_copy(sbuf.at[SELF], abuf.at[SELF], self_sem.at[0])
    self_copy.start()

    sends = loops()

    def each(g, act_on):
        for first, count, pattern in sends[g]:

            def one(k, carry, first=first, pattern=pattern):
                act_on(first + k, steps(pattern, k))
                return carry

            lax.fori_loop(0, count - (pattern == "000"), one, 0)

    def send_group(g):
        def send(i, d):
            pltpu.make_async_remote_copy(
                src_ref=sbuf.at[i], dst_ref=abuf.at[i], send_sem=d_send, recv_sem=d_recv.at[g],
                device_id=device(*d), device_id_type=MESH,
            ).start()

        each(g, send)

    send_group(0)
    lax.fori_loop(1, GROUPS, gather, 0)
    for g in range(1, GROUPS):
        send_group(g)

    load_value.wait()
    load_gate.wait()

    def glu_rows(b, carry):
        at = pl.ds(pl.multiple_of(b * 32, 32), 32)
        to = pl.ds(pl.multiple_of(b * 32 + HALO, 32), 32)
        gated = value[at, :].astype(F32) * sigmoid(gate[at, :].astype(F32))
        for l in range(8):
            glu[l, to, :] = gated[:, l * 128 : (l + 1) * 128]
        return carry

    lax.fori_loop(0, 1024 // 32, glu_rows, 0)
    for l in range(8):
        glu[l, pl.ds(1024 + HALO, 8), :] = jnp.zeros((8, 128), F32)

    def conv_block(l, block):
        lanes = pl.ds(pl.multiple_of(l * 128, 128), 128)
        b0 = jnp.minimum(block * CONV_STEP, SEGMENT - CONV_STEP)
        near = [glu[l, pl.ds(b0 + 2 + u, 8, stride=SEGMENT), :] for u in range(CONV_STEP + 30)]
        totals = [None] * CONV_STEP
        for tap in range(31):
            w = jnp.broadcast_to(taps_ref[tap : tap + 1, lanes], (8, 128))
            for b in range(CONV_STEP):
                term = w * near[b + tap]
                totals[b] = term if tap == 0 else totals[b] + term
        for b in range(CONV_STEP):
            conv[l, pl.ds(b0 + b, 8, stride=SEGMENT), :] = totals[b]

    def conv_blocks(first, last):
        def one(n, carry):
            conv_block(n & 7, first + (n >> 3))
            return carry

        lax.fori_loop(0, 8 * (last - first), one, 0)

    for load in small[4:]:
        load.wait()
    conv_blocks(BORDER, BORDER + EARLY)

    for cp in halo_copies:
        cp.wait()
    border = halo[0].astype(F32) * sigmoid(halo[1].astype(F32))
    border = border * jnp.minimum(me, 1).astype(F32)
    for l in range(8):
        glu[l, pl.ds(0, HALO), :] = border[:, l * 128 : (l + 1) * 128]
    conv_blocks(0, BORDER)
    conv_blocks(BORDER + EARLY, CONV_BLOCKS)

    def norm_conv(n, carry):
        at = pl.ds(pl.multiple_of(n * 32, 32), 32)
        v = jnp.concatenate([conv[l, at, :] for l in range(8)], axis=-1)
        center = jnp.mean(v, axis=-1, keepdims=True)
        v = v - center
        spread = jnp.mean(v * v, axis=-1, keepdims=True)
        u = v * lax.rsqrt(spread + 1e-05) * cgain_ref[...] + cshift_ref[...]
        act[at, :] = (u * sigmoid(u)).astype(BF16)
        return carry

    lax.fori_loop(0, 32, norm_conv, 0, unroll=2)

    load_wg.wait()
    load_wu.wait()
    load_wd.wait()

    def group_wait(buf, sem, g):
        n = GSIZE - 1 if g == 0 else GSIZE
        pltpu.make_async_copy(buf.at[pl.ds(0, n)], buf.at[pl.ds(0, n)], sem.at[g]).wait()

    def experts(g):
        unpack(abuf, g * GSIZE)

        def line_up(n, carry):
            cols = pl.ds(pl.multiple_of(n * 128, 128), 128)
            for r in range(CAP):
                rows[pl.ds(r * GSIZE, GSIZE), cols] = scr[pl.ds(r * PIECES + n, GSIZE, stride=PITCH), :].astype(BF16)
            return carry

        lax.fori_loop(0, PIECES, line_up, 0)

        def up(n, carry):
            cols = pl.ds(pl.multiple_of(n * 512, 512), 512)
            pre_gate = jnp.dot(rows[...], wg[:, cols], preferred_element_type=F32)
            pre_up = jnp.dot(rows[...], wu[:, cols], preferred_element_type=F32)
            gated = jnp.minimum(pre_gate, CLAMP_LIMIT)
            lifted = jnp.clip(pre_up, -CLAMP_LIMIT, CLAMP_LIMIT) + 1.0
            hidden[:, cols] = (lifted * gated * sigmoid(GLU_SLOPE * gated)).astype(BF16)
            return carry

        lax.fori_loop(0, 2, up, 0)

        def down(n, carry):
            cols = pl.ds(pl.multiple_of(n * 512, 512), 512)
            spread(jnp.dot(hidden[...], wd[:, cols], preferred_element_type=F32), n * 4)
            return carry

        lax.fori_loop(0, 4, down, 0)
        pack(rbuf, g * GSIZE)

        def give_back(i, d):
            dz, dx, dy, dc = d
            back = last_hbm.at[i - (PEERS - GSIZE)] if g == GROUPS - 1 else tbuf.at[i]
            pltpu.make_async_remote_copy(
                src_ref=rbuf.at[i], dst_ref=back, send_sem=r_send, recv_sem=r_recv.at[g],
                device_id=device(-dz, -dx, -dy, dc), device_id_type=MESH,
            ).start()

        each(g, give_back)

    w_wait(w_recv.at[0], 6)
    for d in range(1, 4):
        for e in range(1, 4):
            w_block(x, origin(d), 1, device(0, e, 0, 0))
            w_block(4 + z, origin(d), 1, device(e, 0, 0, 0))

    self_copy.wait()
    group_wait(abuf, d_recv, 0)
    experts(0)
    self_back = pltpu.make_async_copy(rbuf.at[SELF], tbuf.at[SELF], self_sem.at[1])
    self_back.start()

    for g in range(1, GROUPS):
        group_wait(abuf, d_recv, g)
        experts(g)

    for g in range(GROUPS):
        ranks = rankm[g * GSIZE : (g + 1) * GSIZE, :]
        parts = sharem[g * GSIZE : (g + 1) * GSIZE, :]
        stacked = jnp.concatenate([jnp.where(ranks == float(r), parts, 0.0) for r in range(CAP)], axis=0)
        weights[pl.ds(g * GSIZE * CAP, GSIZE * CAP), :] = stacked.astype(BF16)

    w_wait(w_recv.at[1], 18)
    for d in range(1, 4):
        pltpu.make_async_remote_copy(
            src_ref=wfull.at[:, origin(d), :], dst_ref=wfull.at[:, origin(d), :],
            send_sem=w_send.at[2], recv_sem=w_recv.at[2], device_id=device(0, 0, 0, 1), device_id_type=MESH,
        ).start()
    own_forward.wait()
    w_wait(w_recv.at[2], 24)

    def project(n, carry):
        cols = pl.ds(pl.multiple_of(n * 256, 256), 256)
        for m in range(2):
            at = pl.ds(m * 512, 512)
            obuf[at, cols] = jnp.dot(act[at, :], wfull[n], preferred_element_type=F32).astype(BF16)
        return carry

    lax.fori_loop(0, 8, project, 0)

    store_mixed = pltpu.make_async_copy(obuf, mixed_hbm, out_sem.at[0])
    store_mixed.start()

    self_back.wait()

    def combine(first, n, last):
        at = pl.ds(first * GSIZE * CAP, (last - first) * GSIZE * CAP)
        cols = pl.ds(pl.multiple_of(n * 512, 512), 512)
        return lax.dot_general(
            weights[at, :], result[at, cols], (((0,), (0,)), ((), ())), preferred_element_type=F32
        ), cols

    for g in range(GROUPS - 1):
        group_wait(tbuf, r_recv, g)
        unpack(tbuf, g * GSIZE)

        def line_up_back(n, carry, g=g):
            cols = pl.ds(pl.multiple_of(n * 128, 128), 128)
            for r in range(CAP):
                result[pl.ds((g * CAP + r) * GSIZE, GSIZE), cols] = scr[
                    pl.ds(r * PIECES + n, GSIZE, stride=PITCH), :
                ].astype(BF16)
            return carry

        lax.fori_loop(0, PIECES, line_up_back, 0)
    for n in range(4):
        cols = pl.ds(n * 512, 512)
        acc[:, cols] = weighted(weights[pl.ds(0, LAST), :], result[pl.ds(0, LAST), cols])
    stores = [store_mixed, pltpu.make_async_copy(acc, acc_hbm, out_sem.at[1])]
    stores.append(pltpu.make_async_copy(weights.at[pl.ds(LAST, GSIZE * CAP), :], last_weights_hbm, out_sem.at[2]))
    for store in stores[1:]:
        store.start()
    group_wait(tbuf, r_recv, GROUPS - 1)
    sent = sbuf.at[pl.ds(0, PEERS - 1)]
    pltpu.make_async_copy(sent, sent, d_send).wait()
    pltpu.make_async_copy(sent, sent, r_send).wait()
    w_wait(w_send.at[0], 6)
    w_wait(w_send.at[1], 18)
    w_wait(w_send.at[2], 24)
    for store in stores:
        store.wait()


def finish(
    mixed_in, acc_in, weights_in, last_in, mixed_out, moe_out, mixed, acc, weights, last, scr, rows, moe, sem_in, sem_out
):
    firsts = ((last_in, last), (weights_in, weights), (acc_in, acc))
    firsts = [pltpu.make_async_copy(a, b, sem_in.at[4 + n]) for n, (a, b) in enumerate(firsts)]
    cuts = [pl.ds(n * 256, 256) for n in range(4)]
    reads = [pltpu.make_async_copy(mixed_in.at[at, :], mixed.at[at, :], sem_in.at[n]) for n, at in enumerate(cuts)]
    writes = [pltpu.make_async_copy(mixed.at[at, :], mixed_out.at[at, :], sem_out.at[n]) for n, at in enumerate(cuts)]
    for read in (firsts[0], *reads[:2], *firsts[1:], *reads[2:]):
        read.start()
    firsts[0].wait()

    for read, write in zip(reads[:2], writes[:2]):
        read.wait()
        write.start()

    def unpack(i, carry):
        scr[pl.ds(pl.multiple_of(i * PITCH, 8), BLOCK), :] = last[i].astype(F32)
        return carry

    lax.fori_loop(0, GSIZE, unpack, 0, unroll=4)

    def line_up(n, carry):
        cols = pl.ds(pl.multiple_of(n * 128, 128), 128)
        for r in range(CAP):
            rows[pl.ds(r * GSIZE, GSIZE), cols] = scr[pl.ds(r * PIECES + n, GSIZE, stride=PITCH), :].astype(BF16)
        return carry

    lax.fori_loop(0, PIECES, line_up, 0)
    for read, write in zip(reads[2:], writes[2:]):
        read.wait()
        write.start()
    for first in firsts[1:]:
        first.wait()
    for n in range(4):
        cols = pl.ds(n * 512, 512)
        moe[:, cols] = (acc[:, cols] + weighted(weights[...], rows[:, cols])).astype(BF16)
    store_moe = pltpu.make_async_copy(moe, moe_out, sem_out.at[4])
    store_moe.start()
    for write in (*writes, store_moe):
        write.wait()


def body(
    glu_value, glu_gate, conv_taps, chan_gain, chan_shift, mix_out_weight, moe_input, moe_gain, expert_ids,
    expert_share, expert_gate_weight, expert_up_weight, expert_down_weight,
):
    hbm = pl.BlockSpec(memory_space=pl.ANY)
    dma = pltpu.SemaphoreType.DMA
    made = pl.pallas_call(
        kernel,
        out_shape=(
            jax.ShapeDtypeStruct((1024, 2048), BF16),
            jax.ShapeDtypeStruct((128, 2048), F32),
            jax.ShapeDtypeStruct((GSIZE * CAP, 128), BF16),
            jax.ShapeDtypeStruct((GSIZE, BLOCK, 128), BF16),
        ),
        in_specs=[hbm] * 14,
        out_specs=(hbm,) * 4,
        scratch_shapes=[
            pltpu.VMEM((31, 1024), F32),
            pltpu.VMEM((1, 1024), F32),
            pltpu.VMEM((1, 1024), F32),
            pltpu.VMEM((1, 2048), F32),
            pltpu.VMEM((4, 128), jnp.int32),
            pltpu.VMEM((4, 128), F32),
            pltpu.VMEM((PEERS, 128), jnp.int32),
            pltpu.VMEM((1024, 1024), BF16),
            pltpu.VMEM((1024, 1024), BF16),
            pltpu.VMEM((2, HALO, 1024), BF16),
            pltpu.VMEM((2, HALO, 1024), BF16),
            pltpu.VMEM((8, 1024 + HALO + 8, 128), F32),
            pltpu.VMEM((8, 8 * SEGMENT, 128), F32),
            pltpu.VMEM((1024, 1024), BF16),
            pltpu.VMEM((8, 1024, 256), BF16),
            pltpu.VMEM((1024, 2048), BF16),
            pltpu.VMEM((128, 2048), BF16),
            pltpu.VMEM((128, 2048), BF16),
            pltpu.VMEM((128, PEERS), F32),
            pltpu.VMEM((128, PEERS), F32),
            pltpu.VMEM((PEERS, BLOCK, 128), BF16),
            pltpu.VMEM((PEERS, BLOCK, 128), BF16),
            pltpu.VMEM((PEERS, BLOCK, 128), BF16),
            pltpu.VMEM((PEERS - GSIZE, BLOCK, 128), BF16),
            pltpu.VMEM((GSIZE * PITCH, 128), F32),
            pltpu.VMEM((GSIZE * CAP, 2048), BF16),
            pltpu.VMEM((GSIZE * CAP, 1024), BF16),
            pltpu.VMEM((2048, 1024), BF16),
            pltpu.VMEM((2048, 1024), BF16),
            pltpu.VMEM((1024, 2048), BF16),
            pltpu.VMEM((PEERS * CAP, 2048), BF16),
            pltpu.VMEM((CAP * PEERS, 128), BF16),
            pltpu.VMEM((128, 2048), F32),
            dma((24,)), dma((3,)), dma((2,)), dma((2,)), dma((3,)), dma((3,)), dma, dma,
            dma, dma((GROUPS,)), dma, dma((GROUPS,)), dma((2,)),
        ],
        compiler_params=pltpu.CompilerParams(
            collective_id=0, has_side_effects=True, vmem_limit_bytes=62 * 2**20
        ),
        name="mixer",
    )(
        glu_value, glu_gate, conv_taps, chan_gain.reshape(1, -1), chan_shift.reshape(1, -1), mix_out_weight,
        moe_input, moe_gain.reshape(1, -1), expert_ids.T, expert_share.T, places(),
        expert_gate_weight, expert_up_weight, expert_down_weight,
    )
    return pl.pallas_call(
        finish,
        out_shape=(jax.ShapeDtypeStruct((1024, 2048), BF16), jax.ShapeDtypeStruct((128, 2048), BF16)),
        in_specs=[hbm] * 4,
        out_specs=(hbm, hbm),
        scratch_shapes=[
            *(pltpu.VMEM(array.shape, array.dtype) for array in made),
            pltpu.VMEM((GSIZE * PITCH, 128), F32),
            pltpu.VMEM((GSIZE * CAP, 2048), BF16),
            pltpu.VMEM((128, 2048), BF16),
            dma((7,)), dma((5,)),
        ],
        compiler_params=pltpu.CompilerParams(vmem_limit_bytes=63 * 2**20),
        name="finish",
    )(*made)


def solution(mesh):
    both = ("ep", "tp")
    placed = (
        P(both, None), P(both, None), P(), P(), P(), P("tp", None), P(both, None), P(), P(both, None),
        P(both, None), P(both, None, None), P(both, None, None), P(both, None, None),
    )
    return jax.shard_map(
        body,
        mesh=mesh,
        in_specs=placed,
        out_specs=(P(both, None), P(both, None)),
        check_vma=False,
    )
```
